256 devices in a mesh: grp: 2 (over z), sp: 16 (over y, core), tp: 8 (over x).
Axes of the slice: x: 8, y: 8, z: 2, core: 2. Of those that a mesh axis runs over, the one named last changes fastest.
The devices are a block of a 8x8x16 slice.
Arguments:
- stream: bfloat16 [8192, 2048], P(('grp', 'sp'), 'tp'), parts along dimension 0, may hold values from -6 to 6
- documents: int32 [8192], P(('grp', 'sp')), parts along dimension 0, may hold values from 0 to 7, never falling along the last dimension, each value on 1 to 768 neighbouring positions
- q_weight: bfloat16 [2, 2048, 2048], P(None, 'sp', 'tp'), may hold values from -0.125 to 0.125
- k_weight: bfloat16 [2, 2048, 2048], P(None, 'sp', 'tp'), may hold values from -0.125 to 0.125
- v_weight: bfloat16 [2, 2048, 2048], P(None, 'sp', 'tp'), may hold values from -0.125 to 0.125
- out_weight: bfloat16 [2, 2048, 2048], P(None, 'sp', 'tp'), may hold values from -0.125 to 0.125
- pre_gain: float32 [2, 2048], replicated, may hold values from 0.1 to 1.9
- post_gain: float32 [2, 2048], P(None, 'tp'), may hold values from 0.1 to 1.9
- offset_bias: float32 [2, 32, 15, 31], P(None, 'tp'), may hold values from -3 to 263
Outputs:
- result_stream: bfloat16 [8192, 2048], P(('grp', 'sp'), 'tp'), parts along dimension 0
The draws below stay inside these ranges and needn't reach their ends.
There are 2 independent parts, one for each index of `grp`. The reference program is written for one: setup_inputs(seed, part) draws one part's arguments, and reference() takes and returns one part's arrays. A program takes and returns all parts, laid end to end along the dimension named above; an argument that names none is the same for every part. Nothing has to cross between parts.
All inputs are finite; a program needn't handle non-finite values.
Results may differ from the reference program's by a relative error of at most 0.02.
Values may be sent and summed in bfloat16 or wider, within the bound.
No kernel may reach another device: no remote copies, remote signals or barrier semaphores. Data moves between devices by JAX's collectives and lax.ppermute only.
A program may use at most 128 MiB of HBM per device.

```python
import math
import jax
import jax.numpy as jnp
import numpy as np
from jax import lax

HEADS = 32
HEAD_DIM = 64
D = 2048
GRID_W = 64
NA_ROWS = 8
NA_COLS = 16
LAYERS = 2
TOK_DEV = 256
TOKENS = 4096
N_SP = 16
N_TP = 8


def draw_offset_bias(key, part):
    table_shape = (LAYERS, HEADS, 2 * NA_ROWS - 1, 2 * NA_COLS - 1)
    base_bias = jnp.clip(0.5 * jax.random.normal(jax.random.fold_in(key, 11), table_shape, jnp.float32), -3.0, 3.0)
    return base_bias


def block_scale(rng, dims, shards, low, high):
    def one(position, shards_of):
        draws = jax.random.uniform(jax.random.fold_in(jax.random.fold_in(rng, 6), position), (shards_of,), jnp.float32, low / len(shards), high / len(shards))
        return jnp.repeat(jnp.exp(draws), dims[position] // shards_of).reshape((-1,) + (1,) * (len(dims) - position - 1))

    loudness = one(*shards[0])
    for cut in shards[1:]:
        loudness = loudness * one(*cut)
    return loudness


def split_up(amount, total, most, skew):
    portions = [(1 << 20) // math.isqrt(rank ** skew) + 1 for rank in range(2, amount + 1)]
    rest, given = total - most - (amount - 1), [1] * (amount - 1)
    while rest > 0:
        movable = [i for i in range(amount - 1) if given[i] < most]
        pool, remaining = sum([portions[i] for i in movable]), rest
        for i in movable:
            more = min(most - given[i], max(1, remaining * portions[i] // pool), rest)
            given[i] = given[i] + more
            rest = rest - more
    return np.array([most] + given)


def ragged(stream_key, amount, total, bound, skew):
    if amount == 2:
        one = jax.random.randint(stream_key, (), max(1, total - bound), min(bound, total - 1) + 1)
        return jnp.stack([one, total - one])
    sizes = jnp.asarray(split_up(amount, total, bound, skew), jnp.int32)
    couples = (amount - 1) // 2
    source_of, taker = sizes[1:1 + 2 * couples:2], sizes[2:2 + 2 * couples:2]
    slack = jnp.minimum(source_of - 1, bound - taker)
    moved = jax.random.randint(jax.random.fold_in(stream_key, 1), (couples,), 0, 1 << 20) % (slack + 1)
    sizes = sizes.at[1:1 + 2 * couples:2].set(source_of - moved).at[2:2 + 2 * couples:2].set(taker + moved)
    return sizes[jax.random.permutation(jax.random.fold_in(stream_key, 2), amount)]


def scatter_about(own_key, extent, width, bound, split=(), kind=jnp.bfloat16):
    drawn = jax.random.normal(own_key, extent, jnp.float32) * width
    if len(split) > 0:
        drawn = block_scale(own_key, extent, split, -0.22, 0.18) * drawn
    return jnp.clip(drawn, min=-bound, max=bound).astype(kind)


def setup_inputs(seed: int = 0, part: int = 0) -> dict:
    splits = jax.random.split(jax.random.key(seed), 10)
    own_keys = jax.random.split(jax.random.fold_in(splits[9], part), 10)
    stream = scatter_about(own_keys[0], (TOKENS, D), 1.0, 6.0, ((0, 16), (1, 8)))
    documents = jnp.searchsorted(jnp.cumsum(ragged(own_keys[1], max(2, N_SP // 2), TOKENS, 3 * TOK_DEV, 0)), jnp.arange(TOKENS), side="right").astype(jnp.int32)
    q_weight = scatter_about(splits[2], (LAYERS, D, D), D ** -0.5, 0.125, ((1, 16), (2, 8)))
    k_weight = scatter_about(splits[3], (LAYERS, D, D), D ** -0.5, 0.125, ((1, 16), (2, 8)))
    v_weight = scatter_about(splits[4], (LAYERS, D, D), D ** -0.5, 0.125, ((1, 16), (2, 8)))
    out_weight = scatter_about(splits[5], (LAYERS, D, D), D ** -0.5, 0.125, ((1, 16), (2, 8)))
    pre_gain = jnp.clip(1.0 + 0.18 * jax.random.normal(splits[6], (LAYERS, D), jnp.float32), 0.1, 1.9)
    post_gain = jnp.clip(1.0 + 0.18 * jax.random.normal(splits[7], (LAYERS, D), jnp.float32), 0.1, 1.9)
    offset_bias = draw_offset_bias(jax.random.fold_in(splits[9], 71), part)
    return dict(stream=stream, documents=documents, q_weight=q_weight, k_weight=k_weight, v_weight=v_weight, out_weight=out_weight, pre_gain=pre_gain, post_gain=post_gain, offset_bias=offset_bias)


EPS = 1e-06

def window_attention(queries, key_grid, value_grid, doc_grid, bias_table):
    total_rows = queries.shape[0]
    column_ids = jnp.arange(GRID_W).astype(jnp.int32)
    column_first = jnp.clip(column_ids - NA_COLS // 2, 0, GRID_W - NA_COLS)
    column_fits = (column_ids[None, :] >= column_first[:, None]) & (column_ids[None, :] < column_first[:, None] + NA_COLS)
    column_index = jnp.clip(column_ids[None, :] - column_ids[:, None] + NA_COLS - 1, 0, 2 * NA_COLS - 2)
    column_bias = bias_table[:, :, column_index]
    score_scale = HEAD_DIM ** (-0.5)

    def one_row(grid_row):
        row_start = jnp.clip(grid_row - NA_ROWS // 2, 0, total_rows - NA_ROWS).astype(jnp.int32)
        key_rows = lax.dynamic_slice_in_dim(key_grid, row_start, NA_ROWS, 0).astype(jnp.float32)
        value_rows = lax.dynamic_slice_in_dim(value_grid, row_start, NA_ROWS, 0).astype(jnp.float32)
        key_docs = lax.dynamic_slice_in_dim(doc_grid, row_start, NA_ROWS, 0)
        query_row = lax.dynamic_index_in_dim(queries, grid_row, 0, keepdims=False).astype(jnp.float32)
        query_docs = lax.dynamic_index_in_dim(doc_grid, grid_row, 0, keepdims=False)
        row_index = (row_start + jnp.arange(NA_ROWS).astype(jnp.int32) - grid_row + NA_ROWS - 1).astype(jnp.int32)
        row_bias = jnp.take(column_bias, row_index, axis=1).transpose(0, 2, 1, 3)
        scores = jnp.einsum('qhd,ikhd->hqik', query_row, key_rows) * score_scale + row_bias
        allowed = column_fits[:, None, :] & (key_docs[None, :, :] == query_docs[:, None, None])
        scores = jnp.where(allowed[None], scores, -jnp.inf)
        row_top = lax.optimization_barrier(jnp.max(scores, axis=(2, 3), keepdims=True))
        shifted_exp = jnp.exp(scores - row_top)
        weights = (shifted_exp / lax.optimization_barrier(jnp.sum(shifted_exp, axis=(2, 3), keepdims=True))).astype(jnp.bfloat16)
        return jnp.einsum('hqik,ikhd->qhd', weights.astype(jnp.float32), value_rows).astype(jnp.bfloat16)
    return lax.map(one_row, jnp.arange(total_rows).astype(jnp.int32))

def reference(stream, documents, q_weight, k_weight, v_weight, out_weight, pre_gain, post_gain, offset_bias):
    total_rows = TOKENS // GRID_W
    doc_grid = documents.reshape(total_rows, GRID_W)
    group_width = D // N_TP
    current = stream
    for layer_index in range(LAYERS):
        stream_f32 = current.astype(jnp.float32)
        inverse = lax.rsqrt(lax.optimization_barrier(jnp.mean(stream_f32 * stream_f32, axis=-1, keepdims=True)) + EPS)
        scaled = (stream_f32 * pre_gain[layer_index]).astype(jnp.bfloat16)

        def project(weight):
            product = jnp.dot(scaled, weight, preferred_element_type=jnp.float32) * inverse
            return product.astype(jnp.bfloat16).reshape(total_rows, GRID_W, HEADS, HEAD_DIM)
        attended = window_attention(project(q_weight[layer_index]), project(k_weight[layer_index]), project(v_weight[layer_index]), doc_grid, offset_bias[layer_index])
        attended = attended.reshape(TOKENS, D)
        branch = jnp.zeros((TOKENS, D), jnp.float32)
        for group_index in range(N_TP):
            lower = group_index * group_width
            upper = lower + group_width
            partial_value = jnp.dot(attended[:, lower:upper], out_weight[layer_index][:, lower:upper].T, preferred_element_type=jnp.float32)
            rounded = lax.optimization_barrier(partial_value.astype(jnp.bfloat16))
            branch = branch + rounded.astype(jnp.float32)
        out_inverse = lax.rsqrt(lax.optimization_barrier(jnp.mean(branch * branch, axis=-1, keepdims=True)) + EPS)
        current = (stream_f32 + branch * out_inverse * post_gain[layer_index]).astype(jnp.bfloat16)
    return current
```

```python
import functools

import jax
import jax.numpy as jnp
from jax import lax
from jax.experimental import pallas as pl
from jax.experimental.pallas import tpu as pltpu
from jax.sharding import PartitionSpec as P

HEAD_DIM = 64
D = 2048
GRID_W = 64
NA_ROWS = 8
NA_COLS = 16
LAYERS = 2
HALF_ROWS = NA_ROWS // 2
LANES = 128
PAD_ROWS = 8
MASKED = -1e30

EPS = 1e-06


ANY = pl.BlockSpec(memory_space=pl.ANY)
VMEM = pl.BlockSpec(memory_space=pltpu.VMEM)


def copies_for(x, axis):
    return jnp.broadcast_to(x, (lax.axis_size(axis), *x.shape))


def exchange(x, axis):
    return lax.all_to_all(x, axis, split_axis=0, concat_axis=0, tiled=True)


def partner(x):
    count = lax.axis_size("sp")
    return lax.ppermute(x, "sp", [(i, i ^ 1) for i in range(count)])


def across(x):
    count = lax.axis_size("sp")
    moves = [(i, i + 1) for i in range(1, count - 1, 2)]
    return lax.ppermute(x, "sp", moves + [(j, i) for i, j in moves])


def both_sides(x):
    near, far = partner(x), across(x)
    odd = lax.axis_index("sp") % 2 == 1
    return near, far, odd


def ring(chunk):
    count = lax.axis_size("sp")
    half = count // 2
    up = [(i, (i + 2) % count) for i in range(count)]
    down = [(j, i) for i, j in up]
    slots = {0: chunk}
    left = right = chunk
    for k in range(1, half // 2 + 1):
        left = lax.ppermute(left, "sp", up)
        slots[-k] = left
        if k < half - half // 2:
            right = lax.ppermute(right, "sp", down)
            slots[k] = right
    return slots


def gathered_weights(chunk):
    slots = ring(chunk)
    keys = sorted(slots, key=abs)
    return [(k, slots[k], partner(slots[k])) for k in keys]


def weight_list(weights):
    return [w for _, own, other in weights for w in (own, other)]


def weight_copies(distances, refs, scratch, sems, first, width):
    me = lax.axis_index("sp")
    pairs = lax.axis_size("sp") // 2
    place, parity = me // 2, lax.rem(me, 2)
    rows = refs[0].shape[0]
    copies = []
    for n, k in enumerate(distances):
        base = lax.rem(place + k + pairs, pairs) * 2
        for m, block in enumerate((base + parity, base + 1 - parity)):
            source = refs[2 * n + m].at[:, first : first + width]
            copies.append(
                pltpu.make_async_copy(
                    source,
                    scratch.at[pl.ds(pl.multiple_of(block * rows, rows), rows), :],
                    sems.at[2 * n + m],
                )
            )
    return copies


def prepare_kernel(total_rows, doc_col_ref, doc_row_ref, table_ref, out_ref):
    rows_dev = doc_col_ref.shape[0] // GRID_W
    ext_rows = rows_dev + 2 * HALF_ROWS
    first_row = lax.axis_index("sp") * rows_dev
    shape = (GRID_W, LANES)
    col = lax.broadcasted_iota(jnp.int32, shape, 0)
    lane = lax.broadcasted_iota(jnp.int32, shape, 1)
    upper = lane // GRID_W
    key_col = lane - upper * GRID_W
    col_first = jnp.clip(col - NA_COLS // 2, 0, GRID_W - NA_COLS)
    col_fits = (key_col >= col_first) & (key_col < col_first + NA_COLS)
    masks = {}
    for i in range(rows_dev):
        row_first = jnp.clip(first_row + i - HALF_ROWS, 0, total_rows - NA_ROWS)
        doc_col = doc_col_ref[i * GRID_W : (i + 1) * GRID_W, :]
        for k in range(ext_rows // 2):
            key_row = first_row - HALF_ROWS + 2 * k + upper
            doc_row = doc_row_ref[:, k * LANES : (k + 1) * LANES]
            masks[i, k] = (
                col_fits
                & (key_row >= row_first)
                & (key_row < row_first + NA_ROWS)
                & (doc_row == doc_col)
            )
    heads = table_ref.shape[0]

    def per_head(h, _):
        tiles = []
        for r in range(table_ref.shape[1]):
            line = jnp.broadcast_to(table_ref[h, r : r + 1, :], shape)
            tiles.append(
                pltpu.roll(line, LANES - (NA_COLS - 1), 1, stride=1, stride_axis=0)
            )
        for i in range(rows_dev):
            for k in range(ext_rows // 2):
                tile = tiles[2 * k - i + NA_ROWS - 1 - HALF_ROWS]
                out_ref[h, i * GRID_W : (i + 1) * GRID_W, k * LANES : (k + 1) * LANES] = (
                    jnp.where(masks[i, k], tile, MASKED)
                )
        return 0

    lax.fori_loop(0, heads, per_head, 0)


def prepare(documents, offset_bias):
    tokens = documents.shape[0]
    rows_dev = tokens // GRID_W
    total_rows = rows_dev * lax.axis_size("sp")
    near, far, odd = both_sides(documents)
    ext = jnp.concatenate(
        [jnp.where(odd, near, far), documents, jnp.where(odd, far, near)]
    )
    layers, heads, rows, cols = offset_bias.shape
    padded = jnp.pad(offset_bias, ((0, 0), (0, 0), (0, 0), (0, GRID_W - cols)))
    table = jnp.concatenate([padded[:, :, :-1], padded[:, :, 1:]], axis=3)
    table = table.reshape(layers * heads, rows - 1, LANES)
    out = pl.pallas_call(
        functools.partial(prepare_kernel, total_rows),
        out_shape=jax.ShapeDtypeStruct((layers * heads, tokens, 3 * tokens), jnp.float32),
        in_specs=[VMEM] * 3,
        out_specs=VMEM,
        name="prepare",
        cost_estimate=pl.CostEstimate(
            flops=4 * layers * heads * tokens * 3 * tokens,
            bytes_accessed=layers * heads * tokens * 3 * tokens * 4,
            transcendentals=0,
        ),
    )(documents.reshape(tokens, 1), ext.reshape(1, 3 * tokens), table)
    return out.reshape(layers, heads, tokens, 3 * tokens)


def project_kernel(distances, first_layer, tokens, *refs):
    if first_layer:
        x_ref, gain_ref, *refs = refs
    else:
        x_ref, total_ref, gain_ref, *refs = refs
    count = 2 * len(distances)
    w_refs, refs = refs[:count], refs[count:]
    if first_layer:
        q_ref, kv_ref, w_all, scaled, sems = refs
    else:
        q_ref, kv_ref, own_ref, w_all, scaled, new, sems = refs
    width = x_ref.shape[2]
    parts = x_ref.shape[0]
    copies = weight_copies(distances, w_refs, w_all, sems, 0, 3 * width)
    for copy in copies:
        copy.start()
    if not first_layer:
        squares = jnp.zeros((tokens, 1), jnp.float32)
        for j in range(parts):
            total = total_ref[j].astype(jnp.float32)
            squares += jnp.sum(total * total, axis=1, keepdims=True)
        out_inverse = lax.rsqrt(squares / D + EPS)
    squares = jnp.zeros((tokens, 1), jnp.float32)
    for j in range(parts):
        x = x_ref[j, :tokens, :].astype(jnp.float32)
        if not first_layer:
            post = x_ref[j, tokens : tokens + PAD_ROWS, :].astype(jnp.float32)
            post = post[0:1] + post[1:2] + post[2:3]
            x = x + total_ref[j].astype(jnp.float32) * out_inverse * post
            rounded = x.astype(jnp.bfloat16)
            new[j] = rounded
            x = rounded.astype(jnp.float32)
        squares += jnp.sum(x * x, axis=1, keepdims=True)
        scaled[:, j * width : (j + 1) * width] = (x * gain_ref[j]).astype(jnp.bfloat16)
    inverse = lax.rsqrt(squares / D + EPS)
    if not first_layer:
        own_ref[...] = new[lax.axis_index("tp")]
    for copy in copies:
        copy.wait()
    for n in range(3):
        product = jnp.dot(
            scaled[...],
            w_all[:, n * width : (n + 1) * width],
            preferred_element_type=jnp.float32,
        )
        product = (product * inverse).astype(jnp.bfloat16)
        if n == 0:
            q_ref[...] = product * jnp.asarray(HEAD_DIM**-0.5, jnp.bfloat16)
        else:
            kv_ref[:, (n - 1) * width : n * width] = product


def project(x_all, total_all, gain, weights, tokens):
    first_layer = total_all is None
    parts, _, width = x_all.shape
    distances = [k for k, _, _ in weights]
    blocks = weight_list(weights)
    outs = [
        jax.ShapeDtypeStruct((tokens, width), jnp.bfloat16),
        jax.ShapeDtypeStruct((tokens, 2 * width), jnp.bfloat16),
    ]
    scratch = [
        pltpu.VMEM((len(blocks) * blocks[0].shape[0], 3 * width), jnp.bfloat16),
        pltpu.VMEM((tokens, parts * width), jnp.bfloat16),
    ]
    args = [x_all]
    if not first_layer:
        outs.append(jax.ShapeDtypeStruct((tokens, width), jnp.bfloat16))
        scratch.append(pltpu.VMEM((parts, tokens, width), jnp.bfloat16))
        args.append(total_all)
    args.append(gain.reshape(parts, 1, width))
    scratch.append(pltpu.SemaphoreType.DMA((len(blocks),)))
    return pl.pallas_call(
        functools.partial(project_kernel, distances, first_layer, tokens),
        out_shape=outs,
        in_specs=[VMEM] * len(args) + [ANY] * len(blocks),
        out_specs=[VMEM] * len(outs),
        scratch_shapes=scratch,
        name="project",
        cost_estimate=pl.CostEstimate(
            flops=2 * tokens * parts * width * 3 * width,
            bytes_accessed=parts * width * 3 * width * 2,
            transcendentals=0,
        ),
    )(*args, *blocks)


def attend_kernel(distances, first, q_ref, before_ref, own_ref, after_ref, bias_ref, *refs):
    count = 2 * len(distances)
    w_refs, (out_ref, w_all, sems) = refs[:count], refs[count:]
    tokens, width = q_ref.shape
    copies = weight_copies(distances, w_refs, w_all, sems, first, width)
    for copy in copies:
        copy.start()
    sides = (before_ref, own_ref, after_ref)
    lane = lax.broadcasted_iota(jnp.int32, (tokens, LANES), 1)
    lower = lane < HEAD_DIM
    attended = []
    for pair in range(width // LANES):
        lanes = slice(pair * LANES, (pair + 1) * LANES)
        value_lanes = slice(width + pair * LANES, width + (pair + 1) * LANES)
        queries = q_ref[:, lanes]
        results = []
        for half in range(2):
            chosen = jnp.where(lower if half == 0 else ~lower, queries, 0)
            head = 2 * pair + half
            scores = [
                lax.dot_general(
                    chosen,
                    side[:, lanes],
                    (((1,), (1,)), ((), ())),
                    preferred_element_type=jnp.float32,
                )
                + bias_ref[head, :, n * tokens : (n + 1) * tokens]
                for n, side in enumerate(sides)
            ]
            top = jnp.max(
                jnp.maximum(jnp.maximum(scores[0], scores[1]), scores[2]),
                axis=1,
                keepdims=True,
            )
            exps = [jnp.exp(score - top) for score in scores]
            total = jnp.sum(exps[0] + exps[1] + exps[2], axis=1, keepdims=True)
            mixed = sum(
                jnp.dot(
                    e.astype(jnp.bfloat16),
                    side[:, value_lanes],
                    preferred_element_type=jnp.float32,
                )
                for e, side in zip(exps, sides)
            )
            results.append(mixed / total)
        attended.append(jnp.where(lower, results[0], results[1]).astype(jnp.bfloat16))
    attended = jnp.concatenate(attended, axis=1)
    for copy in copies:
        copy.wait()
    for n in range(out_ref.shape[0]):
        out_ref[n] = lax.dot_general(
            attended,
            w_all[n * width : (n + 1) * width, :],
            (((1,), (1,)), ((), ())),
            preferred_element_type=jnp.float32,
        ).astype(jnp.bfloat16)


def attend(queries, before, own, after, bias, weights, first):
    tokens, width = queries.shape
    distances = [k for k, _, _ in weights]
    blocks = weight_list(weights)
    rows = len(blocks) * blocks[0].shape[0]
    heads = width // HEAD_DIM
    return pl.pallas_call(
        functools.partial(attend_kernel, distances, first),
        out_shape=jax.ShapeDtypeStruct((rows // width, tokens, width), jnp.bfloat16),
        in_specs=[VMEM] * 5 + [ANY] * len(blocks),
        out_specs=VMEM,
        scratch_shapes=[
            pltpu.VMEM((rows, width), jnp.bfloat16),
            pltpu.SemaphoreType.DMA((len(blocks),)),
        ],
        name="attend",
        cost_estimate=pl.CostEstimate(
            flops=4 * heads * tokens * 3 * tokens * LANES + 2 * tokens * rows * width,
            bytes_accessed=heads * tokens * 3 * tokens * 4 + rows * width * 2,
            transcendentals=heads * tokens * 3 * tokens,
        ),
    )(queries, before, own, after, bias, *blocks)


def summed_kernel(arrived_ref, out_ref):
    total = jnp.sum(arrived_ref[...].astype(jnp.float32), axis=0).astype(jnp.bfloat16)
    for n in range(out_ref.shape[0]):
        out_ref[n] = total


def summed_copies(arrived):
    return pl.pallas_call(
        summed_kernel,
        out_shape=jax.ShapeDtypeStruct(arrived.shape, arrived.dtype),
        in_specs=[VMEM],
        out_specs=VMEM,
        name="summed",
    )(arrived)


def three_parts(x):
    parts = []
    for _ in range(3):
        part = lax.reduce_precision(x, 8, 7)
        parts.append(part)
        x = x - part
    return [p.astype(jnp.bfloat16) for p in parts]


def shards(
    stream, documents, q_weight, k_weight, v_weight, out_weight, pre_gain, post_gain, offset_bias
):
    tokens, width = stream.shape

    def chunk(layer):
        mats = (q_weight, k_weight, v_weight, out_weight)
        return jnp.concatenate([m[layer] for m in mats], axis=1)

    tail = jnp.stack(three_parts(post_gain[0]))
    tail = jnp.pad(tail, ((0, PAD_ROWS - tail.shape[0]), (0, 0)))
    x_all = exchange(copies_for(jnp.concatenate([stream, tail]), "tp"), "tp")
    weights = gathered_weights(chunk(0))
    bias = prepare(documents, offset_bias)

    def attention(layer, queries, kv, weights):
        near, far, odd = both_sides(kv)
        before = jnp.where(odd, near, far)
        after = jnp.where(odd, far, near)
        return attend(queries, before, kv, after, bias[layer], weights, 3 * width)

    queries, kv = project(x_all, None, pre_gain[0], weights, tokens)
    partial_sums = attention(0, queries, kv, weights)
    partial_sums, next_chunk = lax.optimization_barrier((partial_sums, chunk(1)))
    weights = gathered_weights(next_chunk)
    total_all = exchange(summed_copies(exchange(partial_sums, "tp")), "tp")
    queries, kv, own = project(x_all, total_all, pre_gain[1], weights, tokens)
    partial_sums = attention(1, queries, kv, weights)
    own_total = exchange(partial_sums, "tp").astype(jnp.float32).sum(axis=0)
    squares = jnp.sum(own_total * own_total, axis=-1, keepdims=True)
    squares = exchange(copies_for(squares, "tp"), "tp").sum(axis=0)
    out_inverse = lax.rsqrt(squares / D + EPS)
    return (own.astype(jnp.float32) + own_total * out_inverse * post_gain[1]).astype(
        jnp.bfloat16
    )


def solution(mesh):
    in_specs = (
        P(("grp", "sp"), "tp"),
        P(("grp", "sp")),
        P(None, "sp", "tp"),
        P(None, "sp", "tp"),
        P(None, "sp", "tp"),
        P(None, "sp", "tp"),
        P(),
        P(None, "tp"),
        P(None, "tp", None, None),
    )
    out_specs = P(("grp", "sp"), "tp")
    return jax.shard_map(shards, mesh=mesh, in_specs=in_specs, out_specs=out_specs, check_vma=False)
```

```python
import functools

import jax
import jax.numpy as jnp
from jax import lax
from jax.experimental import pallas as pl
from jax.experimental.pallas import tpu as pltpu
from jax.sharding import PartitionSpec as P

HEAD_DIM = 64
D = 2048
GRID_W = 64
NA_ROWS = 8
NA_COLS = 16
LAYERS = 2
HALF_ROWS = NA_ROWS // 2
LANES = 128
PAD_ROWS = 8
MASKED = -1e30

EPS = 1e-06


VMEM = pl.BlockSpec(memory_space=pltpu.VMEM)


def copies_for(x, axis):
    return jnp.broadcast_to(x, (lax.axis_size(axis), *x.shape))


def exchange(x, axis):
    return lax.all_to_all(x, axis, split_axis=0, concat_axis=0, tiled=True)


def partner(x):
    count = lax.axis_size("sp")
    return lax.ppermute(x, "sp", [(i, i ^ 1) for i in range(count)])


def across(x):
    count = lax.axis_size("sp")
    moves = [(i, i + 1) for i in range(1, count - 1, 2)]
    return lax.ppermute(x, "sp", moves + [(j, i) for i, j in moves])


def ring(chunk, name):
    count = lax.axis_size("sp")
    half = count // 2
    up = [(i, (i + 2) % count) for i in range(count)]
    down = [(j, i) for i, j in up]
    slots = {0: chunk}
    left = right = chunk
    for k in range(1, half // 2 + 1):
        with jax.named_scope(f"{name}_up{k}"):
            left = lax.ppermute(left, "sp", up)
        slots[-k] = left
        if k < half - half // 2:
            with jax.named_scope(f"{name}_down{k}"):
                right = lax.ppermute(right, "sp", down)
            slots[k] = right
    return slots


def with_partner(slots, name):
    weights = []
    for k in sorted(slots, key=abs):
        with jax.named_scope(f"{name}_swap{k}"):
            weights.append((k, slots[k], partner(slots[k])))
    return weights


def weight_list(weights):
    return [w for _, own, other in weights for w in (own, other)]


def place_weights(distances, refs, w_all, first):
    me = lax.axis_index("sp")
    pairs = lax.axis_size("sp") // 2
    place, parity = me // 2, lax.rem(me, 2)
    rows = refs[0].shape[0]
    width = w_all.shape[1]
    for n, k in enumerate(distances):
        base = lax.rem(place + k + pairs, pairs) * 2
        for m, block in enumerate((base + parity, base + 1 - parity)):
            start = pl.multiple_of(block * rows, rows)
            w_all[pl.ds(start, rows), :] = refs[2 * n + m][:, first : first + width]


def prepare_kernel(total_rows, layers, doc_ref, near_ref, far_ref, table_ref, *out_refs):
    tokens = doc_ref.shape[1]
    rows_dev = tokens // GRID_W
    me = lax.axis_index("sp")
    first_row = me * rows_dev
    odd = jnp.full((1, tokens), lax.rem(me, 2), jnp.int32) == 1
    near, own, far = near_ref[...], doc_ref[...], far_ref[...]
    sides = (jnp.where(odd, near, far), own, jnp.where(odd, far, near))
    sides = [side.astype(jnp.float32) for side in sides]
    shape = (GRID_W, LANES)
    col = lax.broadcasted_iota(jnp.int32, shape, 0)
    lane = lax.broadcasted_iota(jnp.int32, shape, 1)
    upper = lane // GRID_W
    key_col = lane - upper * GRID_W
    col_first = jnp.clip(col - NA_COLS // 2, 0, GRID_W - NA_COLS)
    col_fits = (key_col >= col_first) & (key_col < col_first + NA_COLS)
    tiles_side = tokens // LANES
    columns = [
        jnp.broadcast_to(sides[1][:, t * LANES : (t + 1) * LANES], (LANES, LANES)).T
        for t in range(tiles_side)
    ]
    masks = {}
    for i in range(rows_dev):
        row_first = jnp.clip(first_row + i - HALF_ROWS, 0, total_rows - NA_ROWS)
        part = i * GRID_W % LANES
        doc_col = columns[i * GRID_W // LANES][part : part + GRID_W, :]
        for k in range(3 * tiles_side):
            key_row = first_row - HALF_ROWS + 2 * k + upper
            t = k % tiles_side
            doc_row = sides[k // tiles_side][:, t * LANES : (t + 1) * LANES]
            masks[i, k] = (
                col_fits
                & (key_row >= row_first)
                & (key_row < row_first + NA_ROWS)
                & (doc_row == doc_col)
            )
    for layer, out_ref in enumerate(out_refs):

        def per_head(h, carry, layer=layer, out_ref=out_ref):
            lines = [table_ref[layer, h, r : r + 1, :] for r in range(table_ref.shape[2])]
            tiles = []
            for r in range(len(lines) - 1):
                line = lines[r] + pltpu.roll(lines[r + 1], GRID_W, 1)
                line = jnp.broadcast_to(line, shape)
                tiles.append(
                    pltpu.roll(line, LANES - (NA_COLS - 1), 1, stride=1, stride_axis=0)
                )
            for i in range(rows_dev):
                rows = slice(i * GRID_W, (i + 1) * GRID_W)
                for k in range(3 * tiles_side):
                    tile = tiles[2 * k - i + NA_ROWS - 1 - HALF_ROWS]
                    out_ref[h, rows, k * LANES : (k + 1) * LANES] = jnp.where(
                        masks[i, k], tile, MASKED
                    )
            return carry

        lax.fori_loop(0, out_ref.shape[0], per_head, 0)


def prepare(documents, near, far, offset_bias):
    tokens = documents.shape[0]
    total_rows = tokens // GRID_W * lax.axis_size("sp")
    layers, heads, rows, cols = offset_bias.shape
    table = jnp.pad(offset_bias, ((0, 0), (0, 0), (0, 0), (0, LANES - cols)))
    size = heads * tokens * 3 * tokens
    return pl.pallas_call(
        functools.partial(prepare_kernel, total_rows, layers),
        out_shape=[jax.ShapeDtypeStruct((heads, tokens, 3 * tokens), jnp.float32)] * layers,
        in_specs=[VMEM] * 4,
        out_specs=[VMEM] * layers,
        name="prepare",
        compiler_params=pltpu.CompilerParams(vmem_limit_bytes=16 * 2**20),
        cost_estimate=pl.CostEstimate(
            flops=4 * layers * size, bytes_accessed=layers * size * 4, transcendentals=0
        ),
    )(documents.reshape(1, tokens), near.reshape(1, tokens), far.reshape(1, tokens), table)


def scale_kernel(first_layer, tokens, *refs):
    if first_layer:
        x_ref, gain_ref, scaled_ref, inverse_ref = refs
    else:
        x_ref, total_ref, gain_ref, scaled_ref, inverse_ref, own_ref, new = refs
    parts, _, width = x_ref.shape
    if not first_layer:
        squares = jnp.zeros((tokens, 1), jnp.float32)
        for j in range(parts):
            total = total_ref[j].astype(jnp.float32)
            squares += jnp.sum(total * total, axis=1, keepdims=True)
        out_inverse = lax.rsqrt(squares / D + EPS)
    squares = jnp.zeros((tokens, 1), jnp.float32)
    for j in range(parts):
        x = x_ref[j, :tokens, :].astype(jnp.float32)
        if not first_layer:
            post = x_ref[j, tokens : tokens + PAD_ROWS, :].astype(jnp.float32)
            post = post[0:1] + post[1:2] + post[2:3]
            x = x + total_ref[j].astype(jnp.float32) * out_inverse * post
            rounded = x.astype(jnp.bfloat16)
            new[j] = rounded
            x = rounded.astype(jnp.float32)
        squares += jnp.sum(x * x, axis=1, keepdims=True)
        scaled_ref[:, j * width : (j + 1) * width] = (x * gain_ref[j]).astype(jnp.bfloat16)
    inverse_ref[...] = lax.rsqrt(squares / D + EPS)
    if not first_layer:
        own_ref[...] = new[lax.axis_index("tp")]


def scale(x_all, total_all, gain, tokens):
    first_layer = total_all is None
    parts, _, width = x_all.shape
    outs = [
        jax.ShapeDtypeStruct((tokens, parts * width), jnp.bfloat16),
        jax.ShapeDtypeStruct((tokens, 1), jnp.float32),
    ]
    args, scratch = [x_all], []
    if not first_layer:
        outs.append(jax.ShapeDtypeStruct((tokens, width), jnp.bfloat16))
        scratch.append(pltpu.VMEM((parts, tokens, width), jnp.bfloat16))
        args.append(total_all)
    args.append(gain.reshape(parts, 1, width))
    return pl.pallas_call(
        functools.partial(scale_kernel, first_layer, tokens),
        out_shape=outs,
        in_specs=[VMEM] * len(args),
        out_specs=[VMEM] * len(outs),
        scratch_shapes=scratch,
        name="scale",
        compiler_params=pltpu.CompilerParams(vmem_limit_bytes=16 * 2**20),
        cost_estimate=pl.CostEstimate(
            flops=8 * tokens * parts * width,
            bytes_accessed=4 * tokens * parts * width * 2,
            transcendentals=tokens,
        ),
    )(*args)


def project_kernel(distances, firsts, factor, scaled_ref, inverse_ref, *refs):
    if len(firsts) > 1:
        w_refs, (out_ref, w_other, w_all) = refs[:-3], refs[-3:]
        place_weights(distances, w_refs, w_other, firsts[1])
    else:
        w_refs, (out_ref, w_all) = refs[:-2], refs[-2:]
    place_weights(distances, w_refs, w_all, firsts[0])
    product = jnp.dot(scaled_ref[...], w_all[...], preferred_element_type=jnp.float32)
    product = (product * inverse_ref[...]).astype(jnp.bfloat16)
    if factor is not None:
        product = product * jnp.asarray(factor, jnp.bfloat16)
    out_ref[...] = product


def project(scaled, inverse, weights, firsts, width, factor=None):
    tokens = scaled.shape[0]
    blocks = weight_list(weights)
    rows = len(blocks) * blocks[0].shape[0]
    outs = [jax.ShapeDtypeStruct((tokens, width), jnp.bfloat16)]
    outs += [jax.ShapeDtypeStruct((rows, width), jnp.bfloat16)] * (len(firsts) - 1)
    return pl.pallas_call(
        functools.partial(project_kernel, [k for k, _, _ in weights], firsts, factor),
        out_shape=outs,
        in_specs=[VMEM] * (2 + len(blocks)),
        out_specs=[VMEM] * len(outs),
        scratch_shapes=[pltpu.VMEM((rows, width), jnp.bfloat16)],
        name="project",
        compiler_params=pltpu.CompilerParams(vmem_limit_bytes=16 * 2**20),
        cost_estimate=pl.CostEstimate(
            flops=2 * tokens * rows * width,
            bytes_accessed=2 * rows * width * 2,
            transcendentals=0,
        ),
    )(scaled, inverse, *blocks)


def attend_kernel(q_ref, own_ref, near_ref, far_ref, bias_ref, w_ref, out_ref):
    tokens, width = q_ref.shape
    odd = lax.rem(lax.axis_index("sp"), 2)
    sides = ((own_ref, 1), (near_ref, 2 - 2 * odd), (far_ref, 2 * odd))
    lane = lax.broadcasted_iota(jnp.int32, (tokens, LANES), 1)
    lower = lane < HEAD_DIM
    attended = []
    for pair in range(width // LANES):
        lanes = slice(pair * LANES, (pair + 1) * LANES)
        value_lanes = slice(width + pair * LANES, width + (pair + 1) * LANES)
        queries = q_ref[:, lanes]
        results = []
        for half in range(2):
            chosen = jnp.where(lower if half == 0 else ~lower, queries, 0)
            head = 2 * pair + half
            scores = []
            for side, block in sides:
                start = pl.multiple_of(block * tokens, LANES)
                scores.append(
                    lax.dot_general(
                        chosen,
                        side[:, lanes],
                        (((1,), (1,)), ((), ())),
                        preferred_element_type=jnp.float32,
                    )
                    + bias_ref[head, :, pl.ds(start, tokens)]
                )
            top = jnp.max(
                jnp.maximum(jnp.maximum(scores[0], scores[1]), scores[2]),
                axis=1,
                keepdims=True,
            )
            exps = [jnp.exp(score - top) for score in scores]
            total = jnp.sum(exps[0] + exps[1] + exps[2], axis=1, keepdims=True)
            mixed = sum(
                jnp.dot(
                    e.astype(jnp.bfloat16),
                    side[:, value_lanes],
                    preferred_element_type=jnp.float32,
                )
                for e, (side, _) in zip(exps, sides)
            )
            results.append(mixed / total)
        attended.append(jnp.where(lower, results[0], results[1]).astype(jnp.bfloat16))
    attended = jnp.concatenate(attended, axis=1)
    for n in range(out_ref.shape[0]):
        out_ref[n] = lax.dot_general(
            attended,
            w_ref[n * width : (n + 1) * width, :],
            (((1,), (1,)), ((), ())),
            preferred_element_type=jnp.float32,
        ).astype(jnp.bfloat16)


def attend(queries, own, near, far, bias, w_out):
    tokens, width = queries.shape
    rows = w_out.shape[0]
    heads = width // HEAD_DIM
    return pl.pallas_call(
        attend_kernel,
        out_shape=jax.ShapeDtypeStruct((rows // width, tokens, width), jnp.bfloat16),
        in_specs=[VMEM] * 6,
        out_specs=VMEM,
        name="attend",
        compiler_params=pltpu.CompilerParams(vmem_limit_bytes=20 * 2**20),
        cost_estimate=pl.CostEstimate(
            flops=4 * heads * tokens * 3 * tokens * LANES + 2 * tokens * rows * width,
            bytes_accessed=heads * tokens * 3 * tokens * 4 + rows * width * 2,
            transcendentals=heads * tokens * 3 * tokens,
        ),
    )(queries, own, near, far, bias, w_out)


def summed_kernel(arrived_ref, out_ref):
    total = jnp.sum(arrived_ref[...].astype(jnp.float32), axis=0).astype(jnp.bfloat16)
    for n in range(out_ref.shape[0]):
        out_ref[n] = total


def summed_copies(arrived):
    parts, tokens, width = arrived.shape
    spec = pl.BlockSpec((parts, GRID_W, width), lambda i: (0, i, 0))
    return pl.pallas_call(
        summed_kernel,
        grid=(tokens // GRID_W,),
        out_shape=jax.ShapeDtypeStruct(arrived.shape, arrived.dtype),
        in_specs=[spec],
        out_specs=spec,
        name="summed",
        compiler_params=pltpu.CompilerParams(vmem_limit_bytes=8 * 2**20),
        cost_estimate=pl.CostEstimate(
            flops=2 * parts * tokens * width,
            bytes_accessed=4 * parts * tokens * width,
            transcendentals=0,
        ),
    )(arrived)


def spread_kernel(x_ref, gain_ref, out_ref):
    tokens = x_ref.shape[0]
    rest = gain_ref[...]
    rows = []
    for _ in range(3):
        part = rest.astype(jnp.bfloat16)
        rows.append(part.astype(jnp.float32))
        rest = rest - rows[-1]
    index = lax.broadcasted_iota(jnp.int32, (PAD_ROWS, x_ref.shape[1]), 0)
    tail = jnp.where(index == 0, rows[0], jnp.where(index == 1, rows[1], rows[2]))
    tail = jnp.where(index < 3, tail, 0.0).astype(jnp.bfloat16)
    for n in range(out_ref.shape[0]):
        out_ref[n, :tokens, :] = x_ref[...]
        out_ref[n, tokens:, :] = tail


def spread(x, gain, copies):
    tokens, width = x.shape
    return pl.pallas_call(
        spread_kernel,
        out_shape=jax.ShapeDtypeStruct((copies, tokens + PAD_ROWS, width), x.dtype),
        in_specs=[VMEM] * 2,
        out_specs=VMEM,
        name="spread",
        compiler_params=pltpu.CompilerParams(vmem_limit_bytes=8 * 2**20),
        cost_estimate=pl.CostEstimate(
            flops=0, bytes_accessed=2 * copies * tokens * width, transcendentals=0
        ),
    )(x, gain.reshape(1, width))


def shards(
    stream, documents, q_weight, k_weight, v_weight, out_weight, pre_gain, post_gain, offset_bias
):
    tokens, width = stream.shape

    def side_by_side(layer, *mats):
        return jnp.concatenate([m[layer] for m in mats], axis=1)

    with jax.named_scope("docs"):
        doc_near, doc_far = partner(documents), across(documents)
    x_copies = spread(stream, post_gain[0], lax.axis_size("tp"))
    with jax.named_scope("gather_x"):
        x_all = exchange(x_copies, "tp")
    kv_chunk, qo_chunk, doc_near, doc_far = lax.optimization_barrier(
        (
            side_by_side(0, k_weight, v_weight),
            side_by_side(0, q_weight, out_weight),
            doc_near,
            doc_far,
        )
    )
    kv_weights = with_partner(ring(kv_chunk, "kv"), "kv")
    qo_weights = with_partner(ring(qo_chunk, "qo"), "qo")
    biases = prepare(documents, doc_near, doc_far, offset_bias)

    def block(layer, scaled, inverse, kv_weights, qo_weights, q_first):
        (kv,) = project(scaled, inverse, kv_weights, (0,), 2 * width)
        with jax.named_scope("halo_near"):
            near = partner(kv)
        with jax.named_scope("halo_far"):
            far = across(kv)
        queries, w_out = project(
            scaled, inverse, qo_weights, (q_first, q_first + width), width, HEAD_DIM**-0.5
        )
        return attend(queries, kv, near, far, biases[layer], w_out)

    scaled, inverse = scale(x_all, None, pre_gain[0], tokens)
    partial_sums = block(0, scaled, inverse, kv_weights, qo_weights, 0)
    chunk, partial_sums = lax.optimization_barrier(
        (side_by_side(1, k_weight, v_weight, q_weight, out_weight), partial_sums)
    )
    slots = ring(chunk, "second")
    with jax.named_scope("sum0"):
        arrived = exchange(partial_sums, "tp")
    arrived, slots[-2], slots[2] = lax.optimization_barrier((arrived, slots[-2], slots[2]))
    weights = with_partner(slots, "second")
    with jax.named_scope("gather_total"):
        total_all = exchange(summed_copies(arrived), "tp")
    scaled, inverse, own = scale(x_all, total_all, pre_gain[1], tokens)
    partial_sums = block(1, scaled, inverse, weights, weights, 2 * width)
    own_total = exchange(partial_sums, "tp").astype(jnp.float32).sum(axis=0)
    squares = jnp.sum(own_total * own_total, axis=-1, keepdims=True)
    squares = exchange(copies_for(squares, "tp"), "tp").sum(axis=0)
    out_inverse = lax.rsqrt(squares / D + EPS)
    return (own.astype(jnp.float32) + own_total * out_inverse * post_gain[1]).astype(
        jnp.bfloat16
    )


def solution(mesh):
    in_specs = (
        P(("grp", "sp"), "tp"),
        P(("grp", "sp")),
        P(None, "sp", "tp"),
        P(None, "sp", "tp"),
        P(None, "sp", "tp"),
        P(None, "sp", "tp"),
        P(),
        P(None, "tp"),
        P(None, "tp", None, None),
    )
    out_specs = P(("grp", "sp"), "tp")
    return jax.shard_map(shards, mesh=mesh, in_specs=in_specs, out_specs=out_specs, check_vma=False)
```

```python
import functools

import jax
import jax.numpy as jnp
from jax import lax
from jax.experimental import pallas as pl
from jax.experimental.pallas import tpu as pltpu
from jax.sharding import PartitionSpec as P

HEAD_DIM = 64
D = 2048
GRID_W = 64
NA_ROWS = 8
NA_COLS = 16
LAYERS = 2
HALF_ROWS = NA_ROWS // 2
LANES = 128
PAD_ROWS = 8
MASKED = -1e30

EPS = 1e-06


VMEM = pl.BlockSpec(memory_space=pltpu.VMEM)


def copies_for(x, axis):
    return jnp.broadcast_to(x, (lax.axis_size(axis), *x.shape))


def exchange(x, axis):
    return lax.all_to_all(x, axis, split_axis=0, concat_axis=0, tiled=True)


def partner(x):
    count = lax.axis_size("sp")
    return lax.ppermute(x, "sp", [(i, i ^ 1) for i in range(count)])


def across(x):
    count = lax.axis_size("sp")
    moves = [(i, i + 1) for i in range(1, count - 1, 2)]
    return lax.ppermute(x, "sp", moves + [(j, i) for i, j in moves])


def ring(chunk, name):
    count = lax.axis_size("sp")
    half = count // 2
    up = [(i, (i + 2) % count) for i in range(count)]
    down = [(j, i) for i, j in up]
    slots = {0: chunk}
    left = right = chunk
    for k in range(1, half // 2 + 1):
        with jax.named_scope(f"{name}_up{k}"):
            left = lax.ppermute(left, "sp", up)
        slots[-k] = left
        if k < half - half // 2:
            with jax.named_scope(f"{name}_down{k}"):
                right = lax.ppermute(right, "sp", down)
            slots[k] = right
    return slots


def stack_kernel(*refs):
    *in_refs, out_ref = refs
    for n, ref in enumerate(in_refs):
        out_ref[n] = ref[...]


def stacked(arrays):
    rows, width = arrays[0].shape
    return pl.pallas_call(
        stack_kernel,
        out_shape=jax.ShapeDtypeStruct((len(arrays), rows, width), arrays[0].dtype),
        in_specs=[VMEM] * len(arrays),
        out_specs=VMEM,
        name="stack",
        compiler_params=pltpu.CompilerParams(vmem_limit_bytes=8 * 2**20),
        cost_estimate=pl.CostEstimate(
            flops=len(arrays) * rows * width,
            bytes_accessed=4 * len(arrays) * rows * width,
            transcendentals=0,
        ),
    )(*arrays)


def with_partner(slots, name):
    keys = sorted(slots, key=abs)
    early = [k for k in keys if abs(k) < 3]
    late = [k for k in keys if abs(k) >= 3]
    weights = [((k,), 0, slots[k][None]) for k in keys]
    for group in (early, late):
        with jax.named_scope(f"{name}_swap{abs(group[-1])}"):
            weights.append((tuple(group), 1, partner(stacked([slots[k] for k in group]))))
    return weights


def weight_rows(weights):
    return sum(w.shape[0] * w.shape[1] for _, _, w in weights)


def weight_places(weights):
    return [(keys, other) for keys, other, _ in weights]


def place_weights(places, refs, w_all, first):
    me = lax.axis_index("sp")
    pairs = lax.axis_size("sp") // 2
    place, parity = me // 2, lax.rem(me, 2)
    width = w_all.shape[1]
    for (keys, other), ref in zip(places, refs):
        rows = ref.shape[1]
        for n, k in enumerate(keys):
            block = lax.rem(place + k + pairs, pairs) * 2
            block += 1 - parity if other else parity
            start = pl.multiple_of(block * rows, rows)
            w_all[pl.ds(start, rows), :] = ref[n, :, first : first + width]


def prepare_kernel(total_rows, layers, doc_ref, near_ref, far_ref, table_ref, *out_refs):
    tokens = doc_ref.shape[1]
    rows_dev = tokens // GRID_W
    me = lax.axis_index("sp")
    first_row = me * rows_dev
    odd = jnp.full((1, tokens), lax.rem(me, 2), jnp.int32) == 1
    near, own, far = near_ref[...], doc_ref[...], far_ref[...]
    sides = (jnp.where(odd, near, far), own, jnp.where(odd, far, near))
    sides = [side.astype(jnp.float32) for side in sides]
    shape = (GRID_W, LANES)
    col = lax.broadcasted_iota(jnp.int32, shape, 0)
    lane = lax.broadcasted_iota(jnp.int32, shape, 1)
    upper = lane // GRID_W
    key_col = lane - upper * GRID_W
    col_first = jnp.clip(col - NA_COLS // 2, 0, GRID_W - NA_COLS)
    col_fits = (key_col >= col_first) & (key_col < col_first + NA_COLS)
    tiles_side = tokens // LANES
    columns = [
        jnp.broadcast_to(sides[1][:, t * LANES : (t + 1) * LANES], (LANES, LANES)).T
        for t in range(tiles_side)
    ]
    masks = {}
    for i in range(rows_dev):
        row_first = jnp.clip(first_row + i - HALF_ROWS, 0, total_rows - NA_ROWS)
        part = i * GRID_W % LANES
        doc_col = columns[i * GRID_W // LANES][part : part + GRID_W, :]
        for k in range(3 * tiles_side):
            key_row = first_row - HALF_ROWS + 2 * k + upper
            t = k % tiles_side
            doc_row = sides[k // tiles_side][:, t * LANES : (t + 1) * LANES]
            masks[i, k] = (
                col_fits
                & (key_row >= row_first)
                & (key_row < row_first + NA_ROWS)
                & (doc_row == doc_col)
            )
    for layer, out_ref in enumerate(out_refs):

        def per_head(h, carry, layer=layer, out_ref=out_ref):
            lines = [table_ref[layer, h, r : r + 1, :] for r in range(table_ref.shape[2])]
            tiles = []
            for r in range(len(lines) - 1):
                line = lines[r] + pltpu.roll(lines[r + 1], GRID_W, 1)
                line = jnp.broadcast_to(line, shape)
                tiles.append(
                    pltpu.roll(line, LANES - (NA_COLS - 1), 1, stride=1, stride_axis=0)
                )
            for i in range(rows_dev):
                rows = slice(i * GRID_W, (i + 1) * GRID_W)
                for k in range(3 * tiles_side):
                    tile = tiles[2 * k - i + NA_ROWS - 1 - HALF_ROWS]
                    out_ref[h, rows, k * LANES : (k + 1) * LANES] = jnp.where(
                        masks[i, k], tile, MASKED
                    )
            return carry

        lax.fori_loop(0, out_ref.shape[0], per_head, 0)


def prepare(documents, near, far, offset_bias):
    tokens = documents.shape[0]
    total_rows = tokens // GRID_W * lax.axis_size("sp")
    layers, heads, rows, cols = offset_bias.shape
    table = jnp.pad(offset_bias, ((0, 0), (0, 0), (0, 0), (0, LANES - cols)))
    size = heads * tokens * 3 * tokens
    return pl.pallas_call(
        functools.partial(prepare_kernel, total_rows, layers),
        out_shape=[jax.ShapeDtypeStruct((heads, tokens, 3 * tokens), jnp.float32)] * layers,
        in_specs=[VMEM] * 4,
        out_specs=[VMEM] * layers,
        name="prepare",
        compiler_params=pltpu.CompilerParams(vmem_limit_bytes=16 * 2**20),
        cost_estimate=pl.CostEstimate(
            flops=4 * layers * size, bytes_accessed=layers * size * 4, transcendentals=0
        ),
    )(documents.reshape(1, tokens), near.reshape(1, tokens), far.reshape(1, tokens), table)


def scale_kernel(first_layer, tokens, *refs):
    if first_layer:
        x_ref, gain_ref, scaled_ref, inverse_ref = refs
    else:
        x_ref, total_ref, gain_ref, scaled_ref, inverse_ref, own_ref, new = refs
    parts, _, width = x_ref.shape
    if not first_layer:
        squares = jnp.zeros((tokens, 1), jnp.float32)
        for j in range(parts):
            total = total_ref[j].astype(jnp.float32)
            squares += jnp.sum(total * total, axis=1, keepdims=True)
        out_inverse = lax.rsqrt(squares / D + EPS)
    squares = jnp.zeros((tokens, 1), jnp.float32)
    for j in range(parts):
        x = x_ref[j, :tokens, :].astype(jnp.float32)
        if not first_layer:
            post = x_ref[j, tokens : tokens + PAD_ROWS, :].astype(jnp.float32)
            post = post[0:1] + post[1:2] + post[2:3]
            x = x + total_ref[j].astype(jnp.float32) * out_inverse * post
            rounded = x.astype(jnp.bfloat16)
            new[j] = rounded
            x = rounded.astype(jnp.float32)
        squares += jnp.sum(x * x, axis=1, keepdims=True)
        scaled_ref[:, j * width : (j + 1) * width] = (x * gain_ref[j]).astype(jnp.bfloat16)
    inverse_ref[...] = lax.rsqrt(squares / D + EPS)
    if not first_layer:
        own_ref[...] = new[lax.axis_index("tp")]


def scale(x_all, total_all, gain, tokens):
    first_layer = total_all is None
    parts, _, width = x_all.shape
    outs = [
        jax.ShapeDtypeStruct((tokens, parts * width), jnp.bfloat16),
        jax.ShapeDtypeStruct((tokens, 1), jnp.float32),
    ]
    args, scratch = [x_all], []
    if not first_layer:
        outs.append(jax.ShapeDtypeStruct((tokens, width), jnp.bfloat16))
        scratch.append(pltpu.VMEM((parts, tokens, width), jnp.bfloat16))
        args.append(total_all)
    args.append(gain.reshape(parts, 1, width))
    return pl.pallas_call(
        functools.partial(scale_kernel, first_layer, tokens),
        out_shape=outs,
        in_specs=[VMEM] * len(args),
        out_specs=[VMEM] * len(outs),
        scratch_shapes=scratch,
        name="scale",
        compiler_params=pltpu.CompilerParams(vmem_limit_bytes=16 * 2**20),
        cost_estimate=pl.CostEstimate(
            flops=8 * tokens * parts * width,
            bytes_accessed=4 * tokens * parts * width * 2,
            transcendentals=tokens,
        ),
    )(*args)


def project_kernel(places, firsts, factor, scaled_ref, inverse_ref, *refs):
    if len(firsts) > 1:
        w_refs, (out_ref, w_other, w_all) = refs[:-3], refs[-3:]
        place_weights(places, w_refs, w_other, firsts[1])
    else:
        w_refs, (out_ref, w_all) = refs[:-2], refs[-2:]
    place_weights(places, w_refs, w_all, firsts[0])
    product = jnp.dot(scaled_ref[...], w_all[...], preferred_element_type=jnp.float32)
    product = (product * inverse_ref[...]).astype(jnp.bfloat16)
    if factor is not None:
        product = product * jnp.asarray(factor, jnp.bfloat16)
    out_ref[...] = product


def project(scaled, inverse, weights, firsts, width, factor=None):
    tokens = scaled.shape[0]
    blocks = [w for _, _, w in weights]
    rows = weight_rows(weights)
    outs = [jax.ShapeDtypeStruct((tokens, width), jnp.bfloat16)]
    outs += [jax.ShapeDtypeStruct((rows, width), jnp.bfloat16)] * (len(firsts) - 1)
    return pl.pallas_call(
        functools.partial(project_kernel, weight_places(weights), firsts, factor),
        out_shape=outs,
        in_specs=[VMEM] * (2 + len(blocks)),
        out_specs=[VMEM] * len(outs),
        scratch_shapes=[pltpu.VMEM((rows, width), jnp.bfloat16)],
        name="project",
        compiler_params=pltpu.CompilerParams(vmem_limit_bytes=16 * 2**20),
        cost_estimate=pl.CostEstimate(
            flops=2 * tokens * rows * width,
            bytes_accessed=2 * rows * width * 2,
            transcendentals=0,
        ),
    )(scaled, inverse, *blocks)


def attend_kernel(q_ref, own_ref, near_ref, far_ref, bias_ref, w_ref, out_ref):
    tokens, width = q_ref.shape
    odd = lax.rem(lax.axis_index("sp"), 2)
    sides = ((own_ref, 1), (near_ref, 2 - 2 * odd), (far_ref, 2 * odd))
    lane = lax.broadcasted_iota(jnp.int32, (tokens, LANES), 1)
    lower = lane < HEAD_DIM
    attended = []
    for pair in range(width // LANES):
        lanes = slice(pair * LANES, (pair + 1) * LANES)
        value_lanes = slice(width + pair * LANES, width + (pair + 1) * LANES)
        queries = q_ref[:, lanes]
        results = []
        for half in range(2):
            chosen = jnp.where(lower if half == 0 else ~lower, queries, 0)
            head = 2 * pair + half
            scores = []
            for side, block in sides:
                start = pl.multiple_of(block * tokens, LANES)
                scores.append(
                    lax.dot_general(
                        chosen,
                        side[:, lanes],
                        (((1,), (1,)), ((), ())),
                        preferred_element_type=jnp.float32,
                    )
                    + bias_ref[head, :, pl.ds(start, tokens)]
                )
            top = jnp.max(
                jnp.maximum(jnp.maximum(scores[0], scores[1]), scores[2]),
                axis=1,
                keepdims=True,
            )
            exps = [jnp.exp(score - top) for score in scores]
            total = jnp.sum(exps[0] + exps[1] + exps[2], axis=1, keepdims=True)
            mixed = sum(
                jnp.dot(
                    e.astype(jnp.bfloat16),
                    side[:, value_lanes],
                    preferred_element_type=jnp.float32,
                )
                for e, (side, _) in zip(exps, sides)
            )
            results.append(mixed / total)
        attended.append(jnp.where(lower, results[0], results[1]).astype(jnp.bfloat16))
    attended = jnp.concatenate(attended, axis=1)
    for n in range(out_ref.shape[0]):
        out_ref[n] = lax.dot_general(
            attended,
            w_ref[n * width : (n + 1) * width, :],
            (((1,), (1,)), ((), ())),
            preferred_element_type=jnp.float32,
        ).astype(jnp.bfloat16)


def attend(queries, own, near, far, bias, w_out):
    tokens, width = queries.shape
    rows = w_out.shape[0]
    heads = width // HEAD_DIM
    return pl.pallas_call(
        attend_kernel,
        out_shape=jax.ShapeDtypeStruct((rows // width, tokens, width), jnp.bfloat16),
        in_specs=[VMEM] * 6,
        out_specs=VMEM,
        name="attend",
        compiler_params=pltpu.CompilerParams(vmem_limit_bytes=20 * 2**20),
        cost_estimate=pl.CostEstimate(
            flops=4 * heads * tokens * 3 * tokens * LANES + 2 * tokens * rows * width,
            bytes_accessed=heads * tokens * 3 * tokens * 4 + rows * width * 2,
            transcendentals=heads * tokens * 3 * tokens,
        ),
    )(queries, own, near, far, bias, w_out)


def summed_kernel(arrived_ref, out_ref):
    total = jnp.sum(arrived_ref[...].astype(jnp.float32), axis=0).astype(jnp.bfloat16)
    for n in range(out_ref.shape[0]):
        out_ref[n] = total


def summed_copies(arrived):
    parts, tokens, width = arrived.shape
    spec = pl.BlockSpec((parts, GRID_W, width), lambda i: (0, i, 0))
    return pl.pallas_call(
        summed_kernel,
        grid=(tokens // GRID_W,),
        out_shape=jax.ShapeDtypeStruct(arrived.shape, arrived.dtype),
        in_specs=[spec],
        out_specs=spec,
        name="summed",
        compiler_params=pltpu.CompilerParams(vmem_limit_bytes=8 * 2**20),
        cost_estimate=pl.CostEstimate(
            flops=2 * parts * tokens * width,
            bytes_accessed=4 * parts * tokens * width,
            transcendentals=0,
        ),
    )(arrived)


def spread_kernel(x_ref, gain_ref, out_ref):
    tokens = x_ref.shape[0]
    rest = gain_ref[...]
    rows = []
    for _ in range(3):
        part = rest.astype(jnp.bfloat16)
        rows.append(part.astype(jnp.float32))
        rest = rest - rows[-1]
    index = lax.broadcasted_iota(jnp.int32, (PAD_ROWS, x_ref.shape[1]), 0)
    tail = jnp.where(index == 0, rows[0], jnp.where(index == 1, rows[1], rows[2]))
    tail = jnp.where(index < 3, tail, 0.0).astype(jnp.bfloat16)
    for n in range(out_ref.shape[0]):
        out_ref[n, :tokens, :] = x_ref[...]
        out_ref[n, tokens:, :] = tail


def spread(x, gain, copies):
    tokens, width = x.shape
    return pl.pallas_call(
        spread_kernel,
        out_shape=jax.ShapeDtypeStruct((copies, tokens + PAD_ROWS, width), x.dtype),
        in_specs=[VMEM] * 2,
        out_specs=VMEM,
        name="spread",
        compiler_params=pltpu.CompilerParams(vmem_limit_bytes=8 * 2**20),
        cost_estimate=pl.CostEstimate(
            flops=0, bytes_accessed=2 * copies * tokens * width, transcendentals=0
        ),
    )(x, gain.reshape(1, width))


def shards(
    stream, documents, q_weight, k_weight, v_weight, out_weight, pre_gain, post_gain, offset_bias
):
    tokens, width = stream.shape

    def side_by_side(layer):
        mats = (k_weight, v_weight, q_weight, out_weight)
        return jnp.concatenate([m[layer] for m in mats], axis=1)

    with jax.named_scope("docs"):
        doc_near, doc_far = partner(documents), across(documents)
    x_copies = spread(stream, post_gain[0], lax.axis_size("tp"))
    with jax.named_scope("gather_x"):
        x_all = exchange(x_copies, "tp")
    chunk, doc_near, doc_far = lax.optimization_barrier((side_by_side(0), doc_near, doc_far))
    weights = with_partner(ring(chunk, "first"), "first")
    biases = prepare(documents, doc_near, doc_far, offset_bias)

    def block(layer, scaled, inverse, weights):
        (kv,) = project(scaled, inverse, weights, (0,), 2 * width)
        with jax.named_scope("halo_near"):
            near = partner(kv)
        with jax.named_scope("halo_far"):
            far = across(kv)
        queries, w_out = project(
            scaled, inverse, weights, (2 * width, 3 * width), width, HEAD_DIM**-0.5
        )
        return attend(queries, kv, near, far, biases[layer], w_out)

    scaled, inverse = scale(x_all, None, pre_gain[0], tokens)
    partial_sums = block(0, scaled, inverse, weights)
    chunk, partial_sums = lax.optimization_barrier(
        (side_by_side(1), partial_sums)
    )
    slots = ring(chunk, "second")
    with jax.named_scope("sum0"):
        arrived = exchange(partial_sums, "tp")
    arrived, slots[-2], slots[2] = lax.optimization_barrier((arrived, slots[-2], slots[2]))
    weights = with_partner(slots, "second")
    with jax.named_scope("gather_total"):
        total_all = exchange(summed_copies(arrived), "tp")
    scaled, inverse, own = scale(x_all, total_all, pre_gain[1], tokens)
    partial_sums = block(1, scaled, inverse, weights)
    own_total = exchange(partial_sums, "tp").astype(jnp.float32).sum(axis=0)
    squares = jnp.sum(own_total * own_total, axis=-1, keepdims=True)
    squares = exchange(copies_for(squares, "tp"), "tp").sum(axis=0)
    out_inverse = lax.rsqrt(squares / D + EPS)
    return (own.astype(jnp.float32) + own_total * out_inverse * post_gain[1]).astype(
        jnp.bfloat16
    )


def solution(mesh):
    in_specs = (
        P(("grp", "sp"), "tp"),
        P(("grp", "sp")),
        P(None, "sp", "tp"),
        P(None, "sp", "tp"),
        P(None, "sp", "tp"),
        P(None, "sp", "tp"),
        P(),
        P(None, "tp"),
        P(None, "tp", None, None),
    )
    out_specs = P(("grp", "sp"), "tp")
    return jax.shard_map(shards, mesh=mesh, in_specs=in_specs, out_specs=out_specs, check_vma=False)
```

```python
import functools

import jax
import jax.numpy as jnp
from jax import lax
from jax.experimental import pallas as pl
from jax.experimental.pallas import tpu as pltpu
from jax.sharding import PartitionSpec as P


HEAD_DIM = 64
D = 2048
GRID_W = 64
NA_ROWS = 8
NA_COLS = 16
HALF_ROWS = NA_ROWS // 2
LANES = 128
PAD_ROWS = 8
MASKED = -1e30

EPS = 1e-06


VMEM = pl.BlockSpec(memory_space=pltpu.VMEM)


def copies_for(x, axis):
    return jnp.broadcast_to(x, (lax.axis_size(axis), *x.shape))


def exchange(x, axis):
    return lax.all_to_all(x, axis, split_axis=0, concat_axis=0, tiled=True)


def partner(x):
    count = lax.axis_size("sp")
    return lax.ppermute(x, "sp", [(i, i ^ 1) for i in range(count)])


def across(x):
    count = lax.axis_size("sp")
    moves = [(i, i + 1) for i in range(1, count - 1, 2)]
    return lax.ppermute(x, "sp", moves + [(j, i) for i, j in moves])


def ring(chunk):
    count = lax.axis_size("sp")
    half = count // 2
    up = [(i, (i + 2) % count) for i in range(count)]
    down = [(j, i) for i, j in up]
    slots = {0: chunk}
    left = right = chunk
    for k in range(1, half // 2 + 1):
        left = lax.ppermute(left, "sp", up)
        slots[-k] = left
        if k < half - half // 2:
            right = lax.ppermute(right, "sp", down)
            slots[k] = right
    return slots


def stack_kernel(*refs):
    *in_refs, out_ref = refs
    for n, ref in enumerate(in_refs):
        out_ref[n] = ref[...]


def stacked(arrays):
    rows, width = arrays[0].shape
    return pl.pallas_call(
        stack_kernel,
        out_shape=jax.ShapeDtypeStruct((len(arrays), rows, width), arrays[0].dtype),
        in_specs=[VMEM] * len(arrays),
        out_specs=VMEM,
        name="stack",
        compiler_params=pltpu.CompilerParams(vmem_limit_bytes=8 * 2**20),
        cost_estimate=pl.CostEstimate(
            flops=len(arrays) * rows * width,
            bytes_accessed=4 * len(arrays) * rows * width,
            transcendentals=0,
        ),
    )(*arrays)


def with_partner(slots):
    weights = []
    for low, high in ((0, 2), (3, 3), (4, 4)):
        keys = tuple(k for k in sorted(slots, key=abs) if low <= abs(k) <= high)
        own = [slots[k] for k in keys]
        own = stacked(own) if len(own) > 1 else own[0][None]
        weights += [(keys, 0, own), (keys, 1, partner(own))]
    return weights


def weight_rows(weights):
    return sum(w.shape[0] * w.shape[1] for _, _, w in weights)


def weight_places(weights):
    return [(keys, other) for keys, other, _ in weights]


def place_weights(places, refs, w_all, first=0):
    me = lax.axis_index("sp")
    pairs = lax.axis_size("sp") // 2
    place, parity = me // 2, lax.rem(me, 2)
    width = w_all.shape[1]
    for (keys, other), ref in zip(places, refs):
        rows = ref.shape[1]
        for n, k in enumerate(keys):
            block = lax.rem(place + k + pairs, pairs) * 2
            block += 1 - parity if other else parity
            start = pl.multiple_of(block * rows, rows)
            w_all[pl.ds(start, rows), :] = ref[n, :, first : first + width]


def prepare_kernel(total_rows, doc_ref, near_ref, far_ref, table_ref, *out_refs):
    tokens = doc_ref.shape[1]
    rows_dev = tokens // GRID_W
    me = lax.axis_index("sp")
    first_row = me * rows_dev
    odd = jnp.full((1, tokens), lax.rem(me, 2), jnp.int32) == 1
    near, own, far = near_ref[...], doc_ref[...], far_ref[...]
    sides = (jnp.where(odd, near, far), own, jnp.where(odd, far, near))
    sides = [side.astype(jnp.float32) for side in sides]
    shape = (GRID_W, LANES)
    col = lax.broadcasted_iota(jnp.int32, shape, 0)
    lane = lax.broadcasted_iota(jnp.int32, shape, 1)
    upper = lane // GRID_W
    key_col = lane - upper * GRID_W
    col_first = jnp.clip(col - NA_COLS // 2, 0, GRID_W - NA_COLS)
    col_fits = (key_col >= col_first) & (key_col < col_first + NA_COLS)
    tiles_side = tokens // LANES
    columns = [
        jnp.broadcast_to(sides[1][:, t * LANES : (t + 1) * LANES], (LANES, LANES)).T
        for t in range(tiles_side)
    ]
    masks = {}
    for i in range(rows_dev):
        row_first = jnp.clip(first_row + i - HALF_ROWS, 0, total_rows - NA_ROWS)
        part = i * GRID_W % LANES
        doc_col = columns[i * GRID_W // LANES][part : part + GRID_W, :]
        for k in range(3 * tiles_side):
            key_row = first_row - HALF_ROWS + 2 * k + upper
            t = k % tiles_side
            doc_row = sides[k // tiles_side][:, t * LANES : (t + 1) * LANES]
            masks[i, k] = (
                col_fits
                & (key_row >= row_first)
                & (key_row < row_first + NA_ROWS)
                & (doc_row == doc_col)
            )
    for layer, out_ref in enumerate(out_refs):

        def per_head(h, carry, layer=layer, out_ref=out_ref):
            lines = [table_ref[layer, h, r : r + 1, :] for r in range(table_ref.shape[2])]
            tiles = []
            for r in range(len(lines) - 1):
                line = lines[r] + pltpu.roll(lines[r + 1], GRID_W, 1)
                line = jnp.broadcast_to(line, shape)
                tiles.append(
                    pltpu.roll(line, LANES - (NA_COLS - 1), 1, stride=1, stride_axis=0)
                )
            for i in range(rows_dev):
                rows = slice(i * GRID_W, (i + 1) * GRID_W)
                for k in range(3 * tiles_side):
                    tile = tiles[2 * k - i + NA_ROWS - 1 - HALF_ROWS]
                    out_ref[h, rows, k * LANES : (k + 1) * LANES] = jnp.where(
                        masks[i, k], tile, MASKED
                    )
            return carry

        lax.fori_loop(0, out_ref.shape[0], per_head, 0)


def prepare(documents, near, far, offset_bias):
    tokens = documents.shape[0]
    total_rows = tokens // GRID_W * lax.axis_size("sp")
    layers, heads, _, cols = offset_bias.shape
    table = jnp.pad(offset_bias, ((0, 0), (0, 0), (0, 0), (0, LANES - cols)))
    size = heads * tokens * 3 * tokens
    return pl.pallas_call(
        functools.partial(prepare_kernel, total_rows),
        out_shape=[jax.ShapeDtypeStruct((heads, tokens, 3 * tokens), jnp.float32)] * layers,
        in_specs=[VMEM] * 4,
        out_specs=[VMEM] * layers,
        name="prepare",
        compiler_params=pltpu.CompilerParams(vmem_limit_bytes=16 * 2**20),
        cost_estimate=pl.CostEstimate(
            flops=4 * layers * size, bytes_accessed=layers * size * 4, transcendentals=0
        ),
    )(documents.reshape(1, tokens), near.reshape(1, tokens), far.reshape(1, tokens), table)


def scale_kernel(first_layer, tokens, *refs):
    if first_layer:
        x_ref, gain_ref, scaled_ref, inverse_ref = refs
    else:
        x_ref, total_ref, gain_ref, scaled_ref, inverse_ref, own_ref, new = refs
    parts, _, width = x_ref.shape
    if not first_layer:
        squares = jnp.zeros((tokens, 1), jnp.float32)
        for j in range(parts):
            total = total_ref[j].astype(jnp.float32)
            squares += jnp.sum(total * total, axis=1, keepdims=True)
        out_inverse = lax.rsqrt(squares / D + EPS)
    squares = jnp.zeros((tokens, 1), jnp.float32)
    for j in range(parts):
        x = x_ref[j, :tokens, :].astype(jnp.float32)
        if not first_layer:
            post = x_ref[j, tokens : tokens + PAD_ROWS, :].astype(jnp.float32)
            post = post[0:1] + post[1:2] + post[2:3]
            x = x + total_ref[j].astype(jnp.float32) * out_inverse * post
            rounded = x.astype(jnp.bfloat16)
            new[j] = rounded
            x = rounded.astype(jnp.float32)
        squares += jnp.sum(x * x, axis=1, keepdims=True)
        scaled_ref[:, j * width : (j + 1) * width] = (x * gain_ref[j]).astype(jnp.bfloat16)
    inverse_ref[...] = lax.rsqrt(squares / D + EPS)
    if not first_layer:
        own_ref[...] = new[lax.axis_index("tp")]


def scale(x_all, total_all, gain, tokens):
    first_layer = total_all is None
    parts, _, width = x_all.shape
    outs = [
        jax.ShapeDtypeStruct((tokens, parts * width), jnp.bfloat16),
        jax.ShapeDtypeStruct((tokens, 1), jnp.float32),
    ]
    args, scratch = [x_all], []
    if not first_layer:
        outs.append(jax.ShapeDtypeStruct((tokens, width), jnp.bfloat16))
        scratch.append(pltpu.VMEM((parts, tokens, width), jnp.bfloat16))
        args.append(total_all)
    args.append(gain.reshape(parts, 1, width))
    return pl.pallas_call(
        functools.partial(scale_kernel, first_layer, tokens),
        out_shape=outs,
        in_specs=[VMEM] * len(args),
        out_specs=[VMEM] * len(outs),
        scratch_shapes=scratch,
        name="scale",
        compiler_params=pltpu.CompilerParams(vmem_limit_bytes=8 * 2**20),
        cost_estimate=pl.CostEstimate(
            flops=8 * tokens * parts * width,
            bytes_accessed=4 * tokens * parts * width * 2,
            transcendentals=tokens,
        ),
    )(*args)


def project_kernel(places, firsts, factor, scaled_ref, inverse_ref, *refs):
    if len(firsts) > 1:
        w_refs, (out_ref, w_other, w_all) = refs[:-3], refs[-3:]
        place_weights(places, w_refs, w_other, firsts[1])
    else:
        w_refs, (out_ref, w_all) = refs[:-2], refs[-2:]
    place_weights(places, w_refs, w_all, firsts[0])
    product = jnp.dot(scaled_ref[...], w_all[...], preferred_element_type=jnp.float32)
    product = (product * inverse_ref[...]).astype(jnp.bfloat16)
    if factor is not None:
        product = product * jnp.asarray(factor, jnp.bfloat16)
    out_ref[...] = product


def project(scaled, inverse, weights, part, columns, firsts, width, factor=None):
    tokens = scaled.shape[0]
    blocks = [w for _, _, w in weights]
    rows = weight_rows(weights)
    outs = [jax.ShapeDtypeStruct((tokens, width), jnp.bfloat16)]
    outs += [jax.ShapeDtypeStruct((rows, width), jnp.bfloat16)] * (len(firsts) - 1)
    return pl.pallas_call(
        functools.partial(project_kernel, weight_places(weights), firsts, factor),
        grid=(1,),
        out_shape=outs,
        in_specs=[VMEM] * 2
        + [
            pl.BlockSpec((*w.shape[:2], columns), lambda i: (0, 0, part)) for w in blocks
        ],
        out_specs=[VMEM] * len(outs),
        scratch_shapes=[pltpu.VMEM((rows, width), jnp.bfloat16)],
        name="project",
        compiler_params=pltpu.CompilerParams(vmem_limit_bytes=16 * 2**20),
        cost_estimate=pl.CostEstimate(
            flops=2 * tokens * rows * width,
            bytes_accessed=2 * rows * width * 2,
            transcendentals=0,
        ),
    )(scaled, inverse, *blocks)


def attend_kernel(q_ref, own_ref, near_ref, far_ref, bias_ref, w_ref, out_ref):
    tokens, width = q_ref.shape
    odd = lax.rem(lax.axis_index("sp"), 2)
    sides = ((own_ref, 1), (near_ref, 2 - 2 * odd), (far_ref, 2 * odd))
    lane = lax.broadcasted_iota(jnp.int32, (tokens, LANES), 1)
    lower = lane < HEAD_DIM
    attended = []
    for pair in range(width // LANES):
        lanes = slice(pair * LANES, (pair + 1) * LANES)
        value_lanes = slice(width + pair * LANES, width + (pair + 1) * LANES)
        queries = q_ref[:, lanes]
        results = []
        for half in range(2):
            chosen = jnp.where(lower if half == 0 else ~lower, queries, 0)
            head = 2 * pair + half
            scores = []
            for side, block in sides:
                start = pl.multiple_of(block * tokens, LANES)
                scores.append(
                    lax.dot_general(
                        chosen,
                        side[:, lanes],
                        (((1,), (1,)), ((), ())),
                        preferred_element_type=jnp.float32,
                    )
                    + bias_ref[head, :, pl.ds(start, tokens)]
                )
            top = jnp.max(
                jnp.maximum(jnp.maximum(scores[0], scores[1]), scores[2]),
                axis=1,
                keepdims=True,
            )
            exps = [jnp.exp(score - top) for score in scores]
            total = jnp.sum(exps[0] + exps[1] + exps[2], axis=1, keepdims=True)
            mixed = sum(
                jnp.dot(
                    e.astype(jnp.bfloat16),
                    side[:, value_lanes],
                    preferred_element_type=jnp.float32,
                )
                for e, (side, _) in zip(exps, sides)
            )
            results.append(mixed / total)
        attended.append(jnp.where(lower, results[0], results[1]).astype(jnp.bfloat16))
    attended = jnp.concatenate(attended, axis=1)
    for n in range(out_ref.shape[0]):
        out_ref[n] = lax.dot_general(
            attended,
            w_ref[n * width : (n + 1) * width, :],
            (((1,), (1,)), ((), ())),
            preferred_element_type=jnp.float32,
        ).astype(jnp.bfloat16)


def attend(queries, own, near, far, bias, w_out):
    tokens, width = queries.shape
    rows = w_out.shape[0]
    heads = width // HEAD_DIM
    return pl.pallas_call(
        attend_kernel,
        out_shape=jax.ShapeDtypeStruct((rows // width, tokens, width), jnp.bfloat16),
        in_specs=[VMEM] * 6,
        out_specs=VMEM,
        name="attend",
        compiler_params=pltpu.CompilerParams(vmem_limit_bytes=20 * 2**20),
        cost_estimate=pl.CostEstimate(
            flops=4 * heads * tokens * 3 * tokens * LANES + 2 * tokens * rows * width,
            bytes_accessed=heads * tokens * 3 * tokens * 4 + rows * width * 2,
            transcendentals=heads * tokens * 3 * tokens,
        ),
    )(queries, own, near, far, bias, w_out)


def summed_kernel(arrived_ref, out_ref):
    total = jnp.sum(arrived_ref[...].astype(jnp.float32), axis=0).astype(jnp.bfloat16)
    for n in range(out_ref.shape[0]):
        out_ref[n] = total


def summed_copies(arrived):
    parts, tokens, width = arrived.shape
    spec = pl.BlockSpec((parts, GRID_W, width), lambda i: (0, i, 0))
    return pl.pallas_call(
        summed_kernel,
        grid=(tokens // GRID_W,),
        out_shape=jax.ShapeDtypeStruct(arrived.shape, arrived.dtype),
        in_specs=[spec],
        out_specs=spec,
        name="summed",
        compiler_params=pltpu.CompilerParams(vmem_limit_bytes=8 * 2**20),
        cost_estimate=pl.CostEstimate(
            flops=2 * parts * tokens * width,
            bytes_accessed=4 * parts * tokens * width,
            transcendentals=0,
        ),
    )(arrived)


def spread_kernel(x_ref, gain_ref, out_ref):
    tokens = x_ref.shape[0]
    rest = gain_ref[...]
    rows = []
    for _ in range(3):
        part = rest.astype(jnp.bfloat16)
        rows.append(part.astype(jnp.float32))
        rest = rest - rows[-1]
    index = lax.broadcasted_iota(jnp.int32, (PAD_ROWS, x_ref.shape[1]), 0)
    tail = jnp.where(index == 0, rows[0], jnp.where(index == 1, rows[1], rows[2]))
    tail = jnp.where(index < 3, tail, 0.0).astype(jnp.bfloat16)
    for n in range(out_ref.shape[0]):
        out_ref[n, :tokens, :] = x_ref[...]
        out_ref[n, tokens:, :] = tail


def spread(x, gain, copies):
    tokens, width = x.shape
    return pl.pallas_call(
        spread_kernel,
        out_shape=jax.ShapeDtypeStruct((copies, tokens + PAD_ROWS, width), x.dtype),
        in_specs=[VMEM] * 2,
        out_specs=VMEM,
        name="spread",
        compiler_params=pltpu.CompilerParams(vmem_limit_bytes=8 * 2**20),
        cost_estimate=pl.CostEstimate(
            flops=0, bytes_accessed=2 * copies * tokens * width, transcendentals=0
        ),
    )(x, gain.reshape(1, width))


def layers(
    stream, documents, q_weight, k_weight, v_weight, out_weight, pre_gain, post_gain, offset_bias
):
    tokens, width = stream.shape

    def side_by_side(layer):
        mats = (k_weight, v_weight, q_weight, out_weight)
        return jnp.concatenate([m[layer] for m in mats], axis=1)

    doc_near, doc_far = partner(documents), across(documents)
    x_copies = spread(stream, post_gain[0], lax.axis_size("tp"))
    x_all = exchange(x_copies, "tp")
    chunk, doc_near, doc_far = lax.optimization_barrier((side_by_side(0), doc_near, doc_far))
    biases = prepare(documents, doc_near, doc_far, offset_bias)
    slots = ring(chunk)
    weights = with_partner(slots)

    def block(layer, scaled, inverse, weights):
        (kv,) = project(scaled, inverse, weights, 0, 2 * width, (0,), 2 * width)
        near = partner(kv)
        far = across(kv)
        queries, w_out = project(
            scaled, inverse, weights, 1, 2 * width, (0, width), width, HEAD_DIM**-0.5
        )
        return attend(queries, kv, near, far, biases[layer], w_out)

    scaled, inverse = scale(x_all, None, pre_gain[0], tokens)
    partial_sums = block(0, scaled, inverse, weights)
    chunk, partial_sums = lax.optimization_barrier(
        (side_by_side(1), partial_sums)
    )
    slots = ring(chunk)
    arrived = exchange(partial_sums, "tp")
    arrived, slots[-2], slots[2] = lax.optimization_barrier((arrived, slots[-2], slots[2]))
    weights = with_partner(slots)
    total_all = exchange(summed_copies(arrived), "tp")
    scaled, inverse, own = scale(x_all, total_all, pre_gain[1], tokens)
    partial_sums = block(1, scaled, inverse, weights)
    own_total = exchange(partial_sums, "tp").astype(jnp.float32).sum(axis=0)
    squares = jnp.sum(own_total * own_total, axis=-1, keepdims=True)
    squares = exchange(copies_for(squares, "tp"), "tp").sum(axis=0)
    out_inverse = lax.rsqrt(squares / D + EPS)
    return (own.astype(jnp.float32) + own_total * out_inverse * post_gain[1]).astype(
        jnp.bfloat16
    )


def solution(mesh):
    in_specs = (
        P(("grp", "sp"), "tp"),
        P(("grp", "sp")),
        P(None, "sp", "tp"),
        P(None, "sp", "tp"),
        P(None, "sp", "tp"),
        P(None, "sp", "tp"),
        P(),
        P(None, "tp"),
        P(None, "tp", None, None),
    )
    out_specs = P(("grp", "sp"), "tp")
    return jax.shard_map(layers, mesh=mesh, in_specs=in_specs, out_specs=out_specs, check_vma=False)
```

```python
import functools

import jax
import jax.numpy as jnp
from jax import lax
from jax.experimental import pallas as pl
from jax.experimental.pallas import tpu as pltpu
from jax.sharding import PartitionSpec as P


HEAD_DIM = 64
D = 2048
GRID_W = 64
NA_ROWS = 8
NA_COLS = 16
HALF_ROWS = NA_ROWS // 2
LANES = 128
PAD_ROWS = 8
MASKED = -1e30

EPS = 1e-06


VMEM = pl.BlockSpec(memory_space=pltpu.VMEM)


def copies_for(x, axis):
    return jnp.broadcast_to(x, (lax.axis_size(axis), *x.shape))


def exchange(x, axis):
    return lax.all_to_all(x, axis, split_axis=0, concat_axis=0, tiled=True)


def partner(x):
    count = lax.axis_size("sp")
    return lax.ppermute(x, "sp", [(i, i ^ 1) for i in range(count)])


def across(x):
    count = lax.axis_size("sp")
    moves = [(i, i + 1) for i in range(1, count - 1, 2)]
    return lax.ppermute(x, "sp", moves + [(j, i) for i, j in moves])


def chunk_kernel(*refs):
    *in_refs, out_ref = refs
    width = in_refs[0].shape[2]
    for n, ref in enumerate(in_refs):
        out_ref[:, n * width : (n + 1) * width] = ref[0]


def side_by_side(layer, *mats):
    _, rows, width = mats[0].shape
    return pl.pallas_call(
        chunk_kernel,
        grid=(1,),
        out_shape=jax.ShapeDtypeStruct((rows, len(mats) * width), mats[0].dtype),
        in_specs=[pl.BlockSpec((1, rows, width), lambda i: (layer, 0, 0))] * len(mats),
        out_specs=pl.BlockSpec((rows, len(mats) * width), lambda i: (0, 0)),
        name="chunk",
        compiler_params=pltpu.CompilerParams(vmem_limit_bytes=8 * 2**20),
        cost_estimate=pl.CostEstimate(
            flops=0, bytes_accessed=4 * len(mats) * rows * width, transcendentals=0
        ),
    )(*mats)


def ring(chunk):
    count = lax.axis_size("sp")
    half = count // 2
    up = [(i, (i + 2) % count) for i in range(count)]
    down = [(j, i) for i, j in up]
    slots = {0: chunk}
    left = right = chunk
    last = half // 2
    middle = chunk.shape[0] // 2
    for k in range(1, last + 1):
        if k == last:
            left, right = left[:middle], right[middle:]
        left = lax.ppermute(left, "sp", up)
        right = lax.ppermute(right, "sp", down)
        slots[-k], slots[k] = left, right
    return slots


def stack_kernel(*refs):
    *in_refs, out_ref = refs
    for n, ref in enumerate(in_refs):
        out_ref[n] = ref[...]


def stacked(arrays):
    rows, width = arrays[0].shape
    return pl.pallas_call(
        stack_kernel,
        out_shape=jax.ShapeDtypeStruct((len(arrays), rows, width), arrays[0].dtype),
        in_specs=[VMEM] * len(arrays),
        out_specs=VMEM,
        name="stack",
        compiler_params=pltpu.CompilerParams(vmem_limit_bytes=8 * 2**20),
        cost_estimate=pl.CostEstimate(
            flops=len(arrays) * rows * width,
            bytes_accessed=4 * len(arrays) * rows * width,
            transcendentals=0,
        ),
    )(*arrays)


def with_partner(slots):
    weights = []
    for low, high in ((0, 2), (3, 3), (4, 4)):
        keys = tuple(k for k in sorted(slots, key=abs) if low <= abs(k) <= high)
        own = stacked([slots[k] for k in keys])
        weights += [(keys, 0, own), (keys, 1, partner(own))]
    return weights


def weight_rows(weights):
    return sum(w.shape[0] * w.shape[1] for _, _, w in weights)


def weight_places(weights):
    return [(keys, other) for keys, other, _ in weights]


def place_weights(places, refs, w_all, first=0):
    me = lax.axis_index("sp")
    pairs = lax.axis_size("sp") // 2
    place, parity = me // 2, lax.rem(me, 2)
    width = w_all.shape[1]
    block_rows = w_all.shape[0] // (2 * pairs)
    for (keys, other), ref in zip(places, refs):
        rows = ref.shape[1]
        for n, k in enumerate(keys):
            block = lax.rem(place + k + pairs, pairs) * 2
            block += 1 - parity if other else parity
            offset = block_rows - rows if k > 0 else 0
            start = pl.multiple_of(block * block_rows + offset, rows)
            w_all[pl.ds(start, rows), :] = ref[n, :, first : first + width]


def prepare_kernel(total_rows, doc_ref, near_ref, far_ref, table_ref, *out_refs):
    tokens = doc_ref.shape[1]
    rows_dev = tokens // GRID_W
    me = lax.axis_index("sp")
    first_row = me * rows_dev
    odd = jnp.full((1, tokens), lax.rem(me, 2), jnp.int32) == 1
    near, own, far = near_ref[...], doc_ref[...], far_ref[...]
    sides = (jnp.where(odd, near, far), own, jnp.where(odd, far, near))
    sides = [side.astype(jnp.float32) for side in sides]
    shape = (GRID_W, LANES)
    col = lax.broadcasted_iota(jnp.int32, shape, 0)
    lane = lax.broadcasted_iota(jnp.int32, shape, 1)
    upper = lane // GRID_W
    key_col = lane - upper * GRID_W
    col_first = jnp.clip(col - NA_COLS // 2, 0, GRID_W - NA_COLS)
    col_fits = (key_col >= col_first) & (key_col < col_first + NA_COLS)
    tiles_side = tokens // LANES
    columns = [
        jnp.broadcast_to(sides[1][:, t * LANES : (t + 1) * LANES], (LANES, LANES)).T
        for t in range(tiles_side)
    ]
    masks = {}
    for i in range(rows_dev):
        row_first = jnp.clip(first_row + i - HALF_ROWS, 0, total_rows - NA_ROWS)
        part = i * GRID_W % LANES
        doc_col = columns[i * GRID_W // LANES][part : part + GRID_W, :]
        for k in range(3 * tiles_side):
            key_row = first_row - HALF_ROWS + 2 * k + upper
            t = k % tiles_side
            doc_row = sides[k // tiles_side][:, t * LANES : (t + 1) * LANES]
            masks[i, k] = (
                col_fits
                & (key_row >= row_first)
                & (key_row < row_first + NA_ROWS)
                & (doc_row == doc_col)
            )
    for layer, out_ref in enumerate(out_refs):

        def per_head(h, carry, layer=layer, out_ref=out_ref):
            lines = [table_ref[layer, h, r : r + 1, :] for r in range(table_ref.shape[2])]
            tiles = []
            for r in range(len(lines) - 1):
                line = lines[r] + pltpu.roll(lines[r + 1], GRID_W, 1)
                line = jnp.broadcast_to(line, shape)
                tiles.append(
                    pltpu.roll(line, LANES - (NA_COLS - 1), 1, stride=1, stride_axis=0)
                )
            for i in range(rows_dev):
                rows = slice(i * GRID_W, (i + 1) * GRID_W)
                for k in range(3 * tiles_side):
                    tile = tiles[2 * k - i + NA_ROWS - 1 - HALF_ROWS]
                    out_ref[h, rows, k * LANES : (k + 1) * LANES] = jnp.where(
                        masks[i, k], tile, MASKED
                    )
            return carry

        lax.fori_loop(0, out_ref.shape[0], per_head, 0)


def prepare(documents, near, far, offset_bias):
    tokens = documents.shape[0]
    total_rows = tokens // GRID_W * lax.axis_size("sp")
    layers, heads, _, cols = offset_bias.shape
    table = jnp.pad(offset_bias, ((0, 0), (0, 0), (0, 0), (0, LANES - cols)))
    size = heads * tokens * 3 * tokens
    return pl.pallas_call(
        functools.partial(prepare_kernel, total_rows),
        out_shape=[jax.ShapeDtypeStruct((heads, tokens, 3 * tokens), jnp.float32)] * layers,
        in_specs=[VMEM] * 4,
        out_specs=[VMEM] * layers,
        name="prepare",
        compiler_params=pltpu.CompilerParams(vmem_limit_bytes=16 * 2**20),
        cost_estimate=pl.CostEstimate(
            flops=4 * layers * size, bytes_accessed=layers * size * 4, transcendentals=0
        ),
    )(documents.reshape(1, tokens), near.reshape(1, tokens), far.reshape(1, tokens), table)


def scale_kernel(first_layer, *refs):
    if first_layer:
        x_ref, gain_ref, scaled_ref, inverse_ref = refs
    else:
        x_ref, post_ref, total_ref, gain_ref, scaled_ref, inverse_ref, own_ref, new = refs
    parts, tokens, width = x_ref.shape
    if not first_layer:
        squares = jnp.zeros((tokens, 1), jnp.float32)
        for j in range(parts):
            total = total_ref[j].astype(jnp.float32)
            squares += jnp.sum(total * total, axis=1, keepdims=True)
        out_inverse = lax.rsqrt(squares / D + EPS)
    squares = jnp.zeros((tokens, 1), jnp.float32)
    for j in range(parts):
        x = x_ref[j].astype(jnp.float32)
        if not first_layer:
            post = post_ref[j].astype(jnp.float32)
            post = post[0:1] + post[1:2] + post[2:3]
            x = x + total_ref[j].astype(jnp.float32) * out_inverse * post
            rounded = x.astype(jnp.bfloat16)
            new[j] = rounded
            x = rounded.astype(jnp.float32)
        squares += jnp.sum(x * x, axis=1, keepdims=True)
        scaled_ref[:, j * width : (j + 1) * width] = (x * gain_ref[j]).astype(jnp.bfloat16)
    inverse_ref[...] = lax.rsqrt(squares / D + EPS)
    if not first_layer:
        own_ref[...] = new[lax.axis_index("tp")]


def scale(x_all, total_all, gain, tokens):
    first_layer = total_all is None
    parts, _, width = x_all.shape
    step = GRID_W
    outs = [
        jax.ShapeDtypeStruct((tokens, parts * width), jnp.bfloat16),
        jax.ShapeDtypeStruct((tokens, 1), jnp.float32),
    ]
    out_specs = [
        pl.BlockSpec((step, parts * width), lambda i: (i, 0)),
        pl.BlockSpec((step, 1), lambda i: (i, 0)),
    ]
    args, scratch = [x_all], []
    block = pl.BlockSpec((parts, step, width), lambda i: (0, i, 0))
    in_specs = [block]
    if not first_layer:
        outs.append(jax.ShapeDtypeStruct((tokens, width), jnp.bfloat16))
        out_specs.append(pl.BlockSpec((step, width), lambda i: (i, 0)))
        scratch.append(pltpu.VMEM((parts, step, width), jnp.bfloat16))
        args += [x_all, total_all]
        rows = pl.BlockSpec((parts, PAD_ROWS, width), lambda i: (0, tokens // PAD_ROWS, 0))
        in_specs += [rows, block]
    args.append(gain.reshape(parts, 1, width))
    in_specs.append(pl.BlockSpec((parts, 1, width), lambda i: (0, 0, 0)))
    return pl.pallas_call(
        functools.partial(scale_kernel, first_layer),
        grid=(tokens // step,),
        out_shape=outs,
        in_specs=in_specs,
        out_specs=out_specs,
        scratch_shapes=scratch,
        name="scale",
        compiler_params=pltpu.CompilerParams(vmem_limit_bytes=8 * 2**20),
        cost_estimate=pl.CostEstimate(
            flops=8 * tokens * parts * width,
            bytes_accessed=4 * tokens * parts * width * 2,
            transcendentals=tokens,
        ),
    )(*args)


def project_kernel(places, firsts, factor, scaled_ref, inverse_ref, *refs):
    if len(firsts) > 1:
        w_refs, (out_ref, w_other, w_all) = refs[:-3], refs[-3:]
        place_weights(places, w_refs, w_other, firsts[1])
    else:
        w_refs, (out_ref, w_all) = refs[:-2], refs[-2:]
    place_weights(places, w_refs, w_all, firsts[0])
    product = jnp.dot(scaled_ref[...], w_all[...], preferred_element_type=jnp.float32)
    product = (product * inverse_ref[...]).astype(jnp.bfloat16)
    if factor is not None:
        product = product * jnp.asarray(factor, jnp.bfloat16)
    out_ref[...] = product


def project(scaled, inverse, weights, part, columns, firsts, width, factor=None):
    tokens = scaled.shape[0]
    blocks = [w for _, _, w in weights]
    rows = weight_rows(weights)
    outs = [jax.ShapeDtypeStruct((tokens, width), jnp.bfloat16)]
    outs += [jax.ShapeDtypeStruct((rows, width), jnp.bfloat16)] * (len(firsts) - 1)
    return pl.pallas_call(
        functools.partial(project_kernel, weight_places(weights), firsts, factor),
        grid=(1,),
        out_shape=outs,
        in_specs=[VMEM] * 2
        + [
            pl.BlockSpec((*w.shape[:2], columns), lambda i: (0, 0, part)) for w in blocks
        ],
        out_specs=[VMEM] * len(outs),
        scratch_shapes=[pltpu.VMEM((rows, width), jnp.bfloat16)],
        name="project",
        compiler_params=pltpu.CompilerParams(vmem_limit_bytes=16 * 2**20),
        cost_estimate=pl.CostEstimate(
            flops=2 * tokens * rows * width,
            bytes_accessed=2 * rows * width * 2,
            transcendentals=0,
        ),
    )(scaled, inverse, *blocks)


def attend_kernel(q_ref, own_ref, near_ref, far_ref, bias_ref, w_ref, out_ref):
    tokens, width = q_ref.shape
    odd = lax.rem(lax.axis_index("sp"), 2)
    sides = ((own_ref, 1), (near_ref, 2 - 2 * odd), (far_ref, 2 * odd))
    lane = lax.broadcasted_iota(jnp.int32, (tokens, LANES), 1)
    lower = lane < HEAD_DIM
    attended = []
    for pair in range(width // LANES):
        lanes = slice(pair * LANES, (pair + 1) * LANES)
        value_lanes = slice(width + pair * LANES, width + (pair + 1) * LANES)
        queries = q_ref[:, lanes]
        results = []
        for half in range(2):
            chosen = jnp.where(lower if half == 0 else ~lower, queries, 0)
            head = 2 * pair + half
            scores = []
            for side, block in sides:
                start = pl.multiple_of(block * tokens, LANES)
                scores.append(
                    lax.dot_general(
                        chosen,
                        side[:, lanes],
                        (((1,), (1,)), ((), ())),
                        preferred_element_type=jnp.float32,
                    )
                    + bias_ref[head, :, pl.ds(start, tokens)]
                )
            top = jnp.max(
                jnp.maximum(jnp.maximum(scores[0], scores[1]), scores[2]),
                axis=1,
                keepdims=True,
            )
            exps = [jnp.exp(score - top) for score in scores]
            total = jnp.sum(exps[0] + exps[1] + exps[2], axis=1, keepdims=True)
            mixed = sum(
                jnp.dot(
                    e.astype(jnp.bfloat16),
                    side[:, value_lanes],
                    preferred_element_type=jnp.float32,
                )
                for e, (side, _) in zip(exps, sides)
            )
            results.append(mixed / total)
        attended.append(jnp.where(lower, results[0], results[1]).astype(jnp.bfloat16))
    attended = jnp.concatenate(attended, axis=1)
    for n in range(out_ref.shape[0]):
        out_ref[n] = lax.dot_general(
            attended,
            w_ref[n * width : (n + 1) * width, :],
            (((1,), (1,)), ((), ())),
            preferred_element_type=jnp.float32,
        ).astype(jnp.bfloat16)


def attend(queries, own, near, far, bias, w_out):
    tokens, width = queries.shape
    rows = w_out.shape[0]
    heads = width // HEAD_DIM
    return pl.pallas_call(
        attend_kernel,
        out_shape=jax.ShapeDtypeStruct((rows // width, tokens, width), jnp.bfloat16),
        in_specs=[VMEM] * 6,
        out_specs=VMEM,
        name="attend",
        compiler_params=pltpu.CompilerParams(vmem_limit_bytes=20 * 2**20),
        cost_estimate=pl.CostEstimate(
            flops=4 * heads * tokens * 3 * tokens * LANES + 2 * tokens * rows * width,
            bytes_accessed=heads * tokens * 3 * tokens * 4 + rows * width * 2,
            transcendentals=heads * tokens * 3 * tokens,
        ),
    )(queries, own, near, far, bias, w_out)


def summed_kernel(arrived_ref, out_ref):
    total = jnp.sum(arrived_ref[...].astype(jnp.float32), axis=0).astype(jnp.bfloat16)
    for n in range(out_ref.shape[0]):
        out_ref[n] = total


def summed_copies(arrived):
    parts, tokens, width = arrived.shape
    spec = pl.BlockSpec((parts, GRID_W, width), lambda i: (0, i, 0))
    return pl.pallas_call(
        summed_kernel,
        grid=(tokens // GRID_W,),
        out_shape=jax.ShapeDtypeStruct(arrived.shape, arrived.dtype),
        in_specs=[spec],
        out_specs=spec,
        name="summed",
        compiler_params=pltpu.CompilerParams(vmem_limit_bytes=8 * 2**20),
        cost_estimate=pl.CostEstimate(
            flops=2 * parts * tokens * width,
            bytes_accessed=4 * parts * tokens * width,
            transcendentals=0,
        ),
    )(arrived)


def spread_kernel(x_ref, gain_ref, out_ref):
    tokens = x_ref.shape[0]
    rest = gain_ref[...]
    rows = []
    for _ in range(3):
        part = rest.astype(jnp.bfloat16)
        rows.append(part.astype(jnp.float32))
        rest = rest - rows[-1]
    index = lax.broadcasted_iota(jnp.int32, (PAD_ROWS, x_ref.shape[1]), 0)
    tail = jnp.where(index == 0, rows[0], jnp.where(index == 1, rows[1], rows[2]))
    tail = jnp.where(index < 3, tail, 0.0).astype(jnp.bfloat16)
    for n in range(out_ref.shape[0]):
        out_ref[n, :tokens, :] = x_ref[...]
        out_ref[n, tokens:, :] = tail


def spread(x, gain, copies):
    tokens, width = x.shape
    return pl.pallas_call(
        spread_kernel,
        out_shape=jax.ShapeDtypeStruct((copies, tokens + PAD_ROWS, width), x.dtype),
        in_specs=[VMEM] * 2,
        out_specs=VMEM,
        name="spread",
        compiler_params=pltpu.CompilerParams(vmem_limit_bytes=8 * 2**20),
        cost_estimate=pl.CostEstimate(
            flops=0, bytes_accessed=2 * copies * tokens * width, transcendentals=0
        ),
    )(x, gain.reshape(1, width))


def layers(
    stream, documents, q_weight, k_weight, v_weight, out_weight, pre_gain, post_gain, offset_bias
):
    tokens, width = stream.shape

    mats = (k_weight, v_weight, q_weight, out_weight)
    doc_near, doc_far = partner(documents), across(documents)
    x_copies = spread(stream, post_gain[0], lax.axis_size("tp"))
    x_all = exchange(x_copies, "tp")
    chunk, doc_near, doc_far = lax.optimization_barrier((side_by_side(0, *mats), doc_near, doc_far))
    biases = prepare(documents, doc_near, doc_far, offset_bias)
    slots = ring(chunk)
    weights = with_partner(slots)

    def block(layer, scaled, inverse, weights):
        (kv,) = project(scaled, inverse, weights, 0, 2 * width, (0,), 2 * width)
        near = partner(kv)
        far = across(kv)
        queries, w_out = project(
            scaled, inverse, weights, 1, 2 * width, (0, width), width, HEAD_DIM**-0.5
        )
        return attend(queries, kv, near, far, biases[layer], w_out)

    scaled, inverse = scale(x_all, None, pre_gain[0], tokens)
    partial_sums = block(0, scaled, inverse, weights)
    chunk, partial_sums = lax.optimization_barrier(
        (side_by_side(1, *mats), partial_sums)
    )
    slots = ring(chunk)
    arrived = exchange(partial_sums, "tp")
    arrived, slots[-2], slots[2] = lax.optimization_barrier((arrived, slots[-2], slots[2]))
    weights = with_partner(slots)
    total_all = exchange(summed_copies(arrived), "tp")
    scaled, inverse, own = scale(x_all, total_all, pre_gain[1], tokens)
    partial_sums = block(1, scaled, inverse, weights)
    own_total = exchange(partial_sums, "tp").astype(jnp.float32).sum(axis=0)
    squares = jnp.sum(own_total * own_total, axis=-1, keepdims=True)
    squares = exchange(copies_for(squares, "tp"), "tp").sum(axis=0)
    out_inverse = lax.rsqrt(squares / D + EPS)
    return (own.astype(jnp.float32) + own_total * out_inverse * post_gain[1]).astype(
        jnp.bfloat16
    )


def solution(mesh):
    in_specs = (
        P(("grp", "sp"), "tp"),
        P(("grp", "sp")),
        P(None, "sp", "tp"),
        P(None, "sp", "tp"),
        P(None, "sp", "tp"),
        P(None, "sp", "tp"),
        P(),
        P(None, "tp"),
        P(None, "tp", None, None),
    )
    out_specs = P(("grp", "sp"), "tp")
    return jax.shard_map(layers, mesh=mesh, in_specs=in_specs, out_specs=out_specs, check_vma=False)
```

```python
import functools

import jax
import jax.numpy as jnp
from jax import lax
from jax.experimental import pallas as pl
from jax.experimental.pallas import tpu as pltpu
from jax.sharding import PartitionSpec as P


HEAD_DIM = 64
D = 2048
GRID_W = 64
NA_ROWS = 8
NA_COLS = 16
HALF_ROWS = NA_ROWS // 2
LANES = 128
PAD_ROWS = 8
MASKED = -1e30

EPS = 1e-06


VMEM = pl.BlockSpec(memory_space=pltpu.VMEM)


def copies_for(x, axis):
    return jnp.broadcast_to(x, (lax.axis_size(axis), *x.shape))


def exchange(x, axis):
    return lax.all_to_all(x, axis, split_axis=0, concat_axis=0, tiled=True)


def partner(x):
    count = lax.axis_size("sp")
    return lax.ppermute(x, "sp", [(i, i ^ 1) for i in range(count)])


def across(x):
    count = lax.axis_size("sp")
    moves = [(i, i + 1) for i in range(1, count - 1, 2)]
    return lax.ppermute(x, "sp", moves + [(j, i) for i, j in moves])


def ring(chunk):
    count = lax.axis_size("sp")
    half = count // 2
    up = [(i, (i + 2) % count) for i in range(count)]
    down = [(j, i) for i, j in up]
    slots = {0: chunk}
    left = right = chunk
    last = half // 2
    middle = chunk.shape[0] // 2
    for k in range(1, last + 1):
        if k == last:
            left, right = left[:middle], right[middle:]
        left = lax.ppermute(left, "sp", up)
        right = lax.ppermute(right, "sp", down)
        slots[-k], slots[k] = left, right
    return slots


def stack_kernel(*refs):
    *in_refs, out_ref = refs
    for n, ref in enumerate(in_refs):
        out_ref[n] = ref[...]


def stacked(arrays):
    rows, width = arrays[0].shape
    return pl.pallas_call(
        stack_kernel,
        out_shape=jax.ShapeDtypeStruct((len(arrays), rows, width), arrays[0].dtype),
        in_specs=[VMEM] * len(arrays),
        out_specs=VMEM,
        name="stack",
        compiler_params=pltpu.CompilerParams(vmem_limit_bytes=8 * 2**20),
        cost_estimate=pl.CostEstimate(
            flops=len(arrays) * rows * width,
            bytes_accessed=4 * len(arrays) * rows * width,
            transcendentals=0,
        ),
    )(*arrays)


def with_partner(slots):
    weights = []
    for low, high in ((0, 2), (3, 3), (4, 4)):
        keys = tuple(k for k in sorted(slots, key=abs) if low <= abs(k) <= high)
        own = stacked([slots[k] for k in keys])
        weights += [(keys, 0, own), (keys, 1, partner(own))]
    return weights


def weight_rows(weights):
    return sum(w.shape[0] * w.shape[1] for _, _, w in weights)


def weight_places(weights):
    return [(keys, other) for keys, other, _ in weights]


def place_weights(places, refs, w_all, first=0):
    me = lax.axis_index("sp")
    pairs = lax.axis_size("sp") // 2
    place, parity = me // 2, lax.rem(me, 2)
    width = w_all.shape[1]
    block_rows = w_all.shape[0] // (2 * pairs)
    for (keys, other), ref in zip(places, refs):
        rows = ref.shape[1]
        for n, k in enumerate(keys):
            block = lax.rem(place + k + pairs, pairs) * 2
            block += 1 - parity if other else parity
            offset = block_rows - rows if k > 0 else 0
            start = pl.multiple_of(block * block_rows + offset, rows)
            w_all[pl.ds(start, rows), :] = ref[n, :, first : first + width]


def prepare_kernel(total_rows, doc_ref, near_ref, far_ref, table_ref, *out_refs):
    tokens = doc_ref.shape[1]
    rows_dev = tokens // GRID_W
    me = lax.axis_index("sp")
    first_row = me * rows_dev
    odd = jnp.full((1, tokens), lax.rem(me, 2), jnp.int32) == 1
    near, own, far = near_ref[...], doc_ref[...], far_ref[...]
    sides = (jnp.where(odd, near, far), own, jnp.where(odd, far, near))
    sides = [side.astype(jnp.float32) for side in sides]
    shape = (GRID_W, LANES)
    col = lax.broadcasted_iota(jnp.int32, shape, 0)
    lane = lax.broadcasted_iota(jnp.int32, shape, 1)
    upper = lane // GRID_W
    key_col = lane - upper * GRID_W
    col_first = jnp.clip(col - NA_COLS // 2, 0, GRID_W - NA_COLS)
    col_fits = (key_col >= col_first) & (key_col < col_first + NA_COLS)
    tiles_side = tokens // LANES
    columns = [
        jnp.broadcast_to(sides[1][:, t * LANES : (t + 1) * LANES], (LANES, LANES)).T
        for t in range(tiles_side)
    ]
    masks = {}
    for i in range(rows_dev):
        row_first = jnp.clip(first_row + i - HALF_ROWS, 0, total_rows - NA_ROWS)
        part = i * GRID_W % LANES
        doc_col = columns[i * GRID_W // LANES][part : part + GRID_W, :]
        for k in range(3 * tiles_side):
            key_row = first_row - HALF_ROWS + 2 * k + upper
            t = k % tiles_side
            doc_row = sides[k // tiles_side][:, t * LANES : (t + 1) * LANES]
            masks[i, k] = (
                col_fits
                & (key_row >= row_first)
                & (key_row < row_first + NA_ROWS)
                & (doc_row == doc_col)
            )
    for layer, out_ref in enumerate(out_refs):

        def per_head(h, carry, layer=layer, out_ref=out_ref):
            lines = [table_ref[layer, h, r : r + 1, :] for r in range(table_ref.shape[2])]
            tiles = []
            for r in range(len(lines) - 1):
                line = lines[r] + pltpu.roll(lines[r + 1], GRID_W, 1)
                line = jnp.broadcast_to(line, shape)
                tiles.append(
                    pltpu.roll(line, LANES - (NA_COLS - 1), 1, stride=1, stride_axis=0)
                )
            for i in range(rows_dev):
                rows = slice(i * GRID_W, (i + 1) * GRID_W)
                for k in range(3 * tiles_side):
                    tile = tiles[2 * k - i + NA_ROWS - 1 - HALF_ROWS]
                    out_ref[h, rows, k * LANES : (k + 1) * LANES] = jnp.where(
                        masks[i, k], tile, MASKED
                    )
            return carry

        lax.fori_loop(0, out_ref.shape[0], per_head, 0)


def prepare(documents, near, far, offset_bias):
    tokens = documents.shape[0]
    total_rows = tokens // GRID_W * lax.axis_size("sp")
    layers, heads, _, cols = offset_bias.shape
    table = jnp.pad(offset_bias, ((0, 0), (0, 0), (0, 0), (0, LANES - cols)))
    size = heads * tokens * 3 * tokens
    return pl.pallas_call(
        functools.partial(prepare_kernel, total_rows),
        out_shape=[jax.ShapeDtypeStruct((heads, tokens, 3 * tokens), jnp.float32)] * layers,
        in_specs=[VMEM] * 4,
        out_specs=[VMEM] * layers,
        name="prepare",
        compiler_params=pltpu.CompilerParams(vmem_limit_bytes=16 * 2**20),
        cost_estimate=pl.CostEstimate(
            flops=4 * layers * size, bytes_accessed=layers * size * 4, transcendentals=0
        ),
    )(documents.reshape(1, tokens), near.reshape(1, tokens), far.reshape(1, tokens), table)


def scale_kernel(first_layer, tokens, *refs):
    if first_layer:
        x_ref, gain_ref, scaled_ref, inverse_ref = refs
    else:
        x_ref, total_ref, gain_ref, scaled_ref, inverse_ref, own_ref, new = refs
    parts, _, width = x_ref.shape
    if not first_layer:
        squares = jnp.zeros((tokens, 1), jnp.float32)
        for j in range(parts):
            total = total_ref[j].astype(jnp.float32)
            squares += jnp.sum(total * total, axis=1, keepdims=True)
        out_inverse = lax.rsqrt(squares / D + EPS)
    squares = jnp.zeros((tokens, 1), jnp.float32)
    for j in range(parts):
        x = x_ref[j, :tokens, :].astype(jnp.float32)
        if not first_layer:
            post = x_ref[j, tokens : tokens + PAD_ROWS, :].astype(jnp.float32)
            post = post[0:1] + post[1:2] + post[2:3]
            x = x + total_ref[j].astype(jnp.float32) * out_inverse * post
            rounded = x.astype(jnp.bfloat16)
            new[j] = rounded
            x = rounded.astype(jnp.float32)
        squares += jnp.sum(x * x, axis=1, keepdims=True)
        scaled_ref[:, j * width : (j + 1) * width] = (x * gain_ref[j]).astype(jnp.bfloat16)
    inverse_ref[...] = lax.rsqrt(squares / D + EPS)
    if not first_layer:
        own_ref[...] = new[lax.axis_index("tp")]


def scale(x_all, total_all, gain, tokens):
    first_layer = total_all is None
    parts, _, width = x_all.shape
    outs = [
        jax.ShapeDtypeStruct((tokens, parts * width), jnp.bfloat16),
        jax.ShapeDtypeStruct((tokens, 1), jnp.float32),
    ]
    args, scratch = [x_all], []
    if not first_layer:
        outs.append(jax.ShapeDtypeStruct((tokens, width), jnp.bfloat16))
        scratch.append(pltpu.VMEM((parts, tokens, width), jnp.bfloat16))
        args.append(total_all)
    args.append(gain.reshape(parts, 1, width))
    return pl.pallas_call(
        functools.partial(scale_kernel, first_layer, tokens),
        out_shape=outs,
        in_specs=[VMEM] * len(args),
        out_specs=[VMEM] * len(outs),
        scratch_shapes=scratch,
        name="scale",
        compiler_params=pltpu.CompilerParams(vmem_limit_bytes=8 * 2**20),
        cost_estimate=pl.CostEstimate(
            flops=8 * tokens * parts * width,
            bytes_accessed=4 * tokens * parts * width * 2,
            transcendentals=tokens,
        ),
    )(*args)


def project_kernel(places, firsts, factor, scaled_ref, inverse_ref, *refs):
    if len(firsts) > 1:
        w_refs, (out_ref, w_other, w_all) = refs[:-3], refs[-3:]
        place_weights(places, w_refs, w_other, firsts[1])
    else:
        w_refs, (out_ref, w_all) = refs[:-2], refs[-2:]
    place_weights(places, w_refs, w_all, firsts[0])
    product = jnp.dot(scaled_ref[...], w_all[...], preferred_element_type=jnp.float32)
    product = (product * inverse_ref[...]).astype(jnp.bfloat16)
    if factor is not None:
        product = product * jnp.asarray(factor, jnp.bfloat16)
    out_ref[...] = product


def project(scaled, inverse, weights, part, columns, firsts, width, factor=None):
    tokens = scaled.shape[0]
    blocks = [w for _, _, w in weights]
    rows = weight_rows(weights)
    outs = [jax.ShapeDtypeStruct((tokens, width), jnp.bfloat16)]
    outs += [jax.ShapeDtypeStruct((rows, width), jnp.bfloat16)] * (len(firsts) - 1)
    return pl.pallas_call(
        functools.partial(project_kernel, weight_places(weights), firsts, factor),
        grid=(1,),
        out_shape=outs,
        in_specs=[VMEM] * 2
        + [
            pl.BlockSpec((*w.shape[:2], columns), lambda i: (0, 0, part)) for w in blocks
        ],
        out_specs=[VMEM] * len(outs),
        scratch_shapes=[pltpu.VMEM((rows, width), jnp.bfloat16)],
        name="project",
        compiler_params=pltpu.CompilerParams(vmem_limit_bytes=16 * 2**20),
        cost_estimate=pl.CostEstimate(
            flops=2 * tokens * rows * width,
            bytes_accessed=2 * rows * width * 2,
            transcendentals=0,
        ),
    )(scaled, inverse, *blocks)


def attend_kernel(q_ref, own_ref, near_ref, far_ref, bias_ref, w_ref, out_ref):
    tokens, width = q_ref.shape
    odd = lax.rem(lax.axis_index("sp"), 2)
    sides = ((own_ref, 1), (near_ref, 2 - 2 * odd), (far_ref, 2 * odd))
    lane = lax.broadcasted_iota(jnp.int32, (tokens, LANES), 1)
    lower = lane < HEAD_DIM
    attended = []
    for pair in range(width // LANES):
        lanes = slice(pair * LANES, (pair + 1) * LANES)
        value_lanes = slice(width + pair * LANES, width + (pair + 1) * LANES)
        queries = q_ref[:, lanes]
        results = []
        for half in range(2):
            chosen = jnp.where(lower if half == 0 else ~lower, queries, 0)
            head = 2 * pair + half
            scores = []
            for side, block in sides:
                start = pl.multiple_of(block * tokens, LANES)
                scores.append(
                    lax.dot_general(
                        chosen,
                        side[:, lanes],
                        (((1,), (1,)), ((), ())),
                        preferred_element_type=jnp.float32,
                    )
                    + bias_ref[head, :, pl.ds(start, tokens)]
                )
            top = jnp.max(
                jnp.maximum(jnp.maximum(scores[0], scores[1]), scores[2]),
                axis=1,
                keepdims=True,
            )
            exps = [jnp.exp(score - top) for score in scores]
            total = jnp.sum(exps[0] + exps[1] + exps[2], axis=1, keepdims=True)
            mixed = sum(
                jnp.dot(
                    e.astype(jnp.bfloat16),
                    side[:, value_lanes],
                    preferred_element_type=jnp.float32,
                )
                for e, (side, _) in zip(exps, sides)
            )
            results.append(mixed / total)
        attended.append(jnp.where(lower, results[0], results[1]).astype(jnp.bfloat16))
    attended = jnp.concatenate(attended, axis=1)
    for n in range(out_ref.shape[0]):
        out_ref[n] = lax.dot_general(
            attended,
            w_ref[n * width : (n + 1) * width, :],
            (((1,), (1,)), ((), ())),
            preferred_element_type=jnp.float32,
        ).astype(jnp.bfloat16)


def attend(queries, own, near, far, bias, w_out):
    tokens, width = queries.shape
    rows = w_out.shape[0]
    heads = width // HEAD_DIM
    return pl.pallas_call(
        attend_kernel,
        out_shape=jax.ShapeDtypeStruct((rows // width, tokens, width), jnp.bfloat16),
        in_specs=[VMEM] * 6,
        out_specs=VMEM,
        name="attend",
        compiler_params=pltpu.CompilerParams(vmem_limit_bytes=20 * 2**20),
        cost_estimate=pl.CostEstimate(
            flops=4 * heads * tokens * 3 * tokens * LANES + 2 * tokens * rows * width,
            bytes_accessed=heads * tokens * 3 * tokens * 4 + rows * width * 2,
            transcendentals=heads * tokens * 3 * tokens,
        ),
    )(queries, own, near, far, bias, w_out)


def summed_kernel(arrived_ref, out_ref):
    total = jnp.sum(arrived_ref[...].astype(jnp.float32), axis=0).astype(jnp.bfloat16)
    for n in range(out_ref.shape[0]):
        out_ref[n] = total


def summed_copies(arrived):
    parts, tokens, width = arrived.shape
    spec = pl.BlockSpec((parts, GRID_W, width), lambda i: (0, i, 0))
    return pl.pallas_call(
        summed_kernel,
        grid=(tokens // GRID_W,),
        out_shape=jax.ShapeDtypeStruct(arrived.shape, arrived.dtype),
        in_specs=[spec],
        out_specs=spec,
        name="summed",
        compiler_params=pltpu.CompilerParams(vmem_limit_bytes=8 * 2**20),
        cost_estimate=pl.CostEstimate(
            flops=2 * parts * tokens * width,
            bytes_accessed=4 * parts * tokens * width,
            transcendentals=0,
        ),
    )(arrived)


def spread_kernel(x_ref, gain_ref, out_ref):
    tokens = x_ref.shape[0]
    rest = gain_ref[...]
    rows = []
    for _ in range(3):
        part = rest.astype(jnp.bfloat16)
        rows.append(part.astype(jnp.float32))
        rest = rest - rows[-1]
    index = lax.broadcasted_iota(jnp.int32, (PAD_ROWS, x_ref.shape[1]), 0)
    tail = jnp.where(index == 0, rows[0], jnp.where(index == 1, rows[1], rows[2]))
    tail = jnp.where(index < 3, tail, 0.0).astype(jnp.bfloat16)
    for n in range(out_ref.shape[0]):
        out_ref[n, :tokens, :] = x_ref[...]
        out_ref[n, tokens:, :] = tail


def spread(x, gain, copies):
    tokens, width = x.shape
    return pl.pallas_call(
        spread_kernel,
        out_shape=jax.ShapeDtypeStruct((copies, tokens + PAD_ROWS, width), x.dtype),
        in_specs=[VMEM] * 2,
        out_specs=VMEM,
        name="spread",
        compiler_params=pltpu.CompilerParams(vmem_limit_bytes=8 * 2**20),
        cost_estimate=pl.CostEstimate(
            flops=0, bytes_accessed=2 * copies * tokens * width, transcendentals=0
        ),
    )(x, gain.reshape(1, width))


def layers(
    stream, documents, q_weight, k_weight, v_weight, out_weight, pre_gain, post_gain, offset_bias
):
    tokens, width = stream.shape

    def side_by_side(layer):
        mats = (k_weight, v_weight, q_weight, out_weight)
        return jnp.concatenate([m[layer] for m in mats], axis=1)

    doc_near, doc_far = partner(documents), across(documents)
    x_copies = spread(stream, post_gain[0], lax.axis_size("tp"))
    x_all = exchange(x_copies, "tp")
    chunk, doc_near, doc_far = lax.optimization_barrier((side_by_side(0), doc_near, doc_far))
    biases = prepare(documents, doc_near, doc_far, offset_bias)
    slots = ring(chunk)
    weights = with_partner(slots)

    def block(layer, scaled, inverse, weights):
        (kv,) = project(scaled, inverse, weights, 0, 2 * width, (0,), 2 * width)
        near = partner(kv)
        far = across(kv)
        queries, w_out = project(
            scaled, inverse, weights, 1, 2 * width, (0, width), width, HEAD_DIM**-0.5
        )
        return attend(queries, kv, near, far, biases[layer], w_out)

    scaled, inverse = scale(x_all, None, pre_gain[0], tokens)
    partial_sums = block(0, scaled, inverse, weights)
    chunk, partial_sums = lax.optimization_barrier(
        (side_by_side(1), partial_sums)
    )
    slots = ring(chunk)
    arrived = exchange(partial_sums, "tp")
    arrived, slots[-2], slots[2] = lax.optimization_barrier((arrived, slots[-2], slots[2]))
    weights = with_partner(slots)
    total_all = exchange(summed_copies(arrived), "tp")
    scaled, inverse, own = scale(x_all, total_all, pre_gain[1], tokens)
    partial_sums = block(1, scaled, inverse, weights)
    own_total = exchange(partial_sums, "tp").astype(jnp.float32).sum(axis=0)
    squares = jnp.sum(own_total * own_total, axis=-1, keepdims=True)
    squares = exchange(copies_for(squares, "tp"), "tp").sum(axis=0)
    out_inverse = lax.rsqrt(squares / D + EPS)
    return (own.astype(jnp.float32) + own_total * out_inverse * post_gain[1]).astype(
        jnp.bfloat16
    )


def solution(mesh):
    in_specs = (
        P(("grp", "sp"), "tp"),
        P(("grp", "sp")),
        P(None, "sp", "tp"),
        P(None, "sp", "tp"),
        P(None, "sp", "tp"),
        P(None, "sp", "tp"),
        P(),
        P(None, "tp"),
        P(None, "tp", None, None),
    )
    out_specs = P(("grp", "sp"), "tp")
    return jax.shard_map(layers, mesh=mesh, in_specs=in_specs, out_specs=out_specs, check_vma=False)
```

```python
import functools

import jax
import jax.numpy as jnp
from jax import lax
from jax.experimental import pallas as pl
from jax.experimental.pallas import tpu as pltpu
from jax.sharding import PartitionSpec as P


HEAD_DIM = 64
D = 2048
GRID_W = 64
NA_ROWS = 8
NA_COLS = 16
HALF_ROWS = NA_ROWS // 2
LANES = 128
PAD_ROWS = 8
MASKED = -1e30

EPS = 1e-06


VMEM = pl.BlockSpec(memory_space=pltpu.VMEM)


def copies_for(x, axis):
    return jnp.broadcast_to(x, (lax.axis_size(axis), *x.shape))


def exchange(x, axis):
    return lax.all_to_all(x, axis, split_axis=0, concat_axis=0, tiled=True)


def partner(x):
    count = lax.axis_size("sp")
    return lax.ppermute(x, "sp", [(i, i ^ 1) for i in range(count)])


def across(x):
    count = lax.axis_size("sp")
    moves = [(i, i + 1) for i in range(1, count - 1, 2)]
    return lax.ppermute(x, "sp", moves + [(j, i) for i, j in moves])


def ring(chunk):
    count = lax.axis_size("sp")
    half = count // 2
    up = [(i, (i + 2) % count) for i in range(count)]
    down = [(j, i) for i, j in up]
    slots = {0: chunk}
    left = right = chunk
    last = half // 2
    middle = chunk.shape[0] // 2
    for k in range(1, last + 1):
        if k == last:
            left, right = left[:middle], right[middle:]
        left = lax.ppermute(left, "sp", up)
        right = lax.ppermute(right, "sp", down)
        slots[-k], slots[k] = left, right
    return slots


def stack_kernel(*refs):
    *in_refs, out_ref = refs
    for n, ref in enumerate(in_refs):
        out_ref[n] = ref[...]


def stacked(arrays):
    rows, width = arrays[0].shape
    return pl.pallas_call(
        stack_kernel,
        out_shape=jax.ShapeDtypeStruct((len(arrays), rows, width), arrays[0].dtype),
        in_specs=[VMEM] * len(arrays),
        out_specs=VMEM,
        name="stack",
        compiler_params=pltpu.CompilerParams(vmem_limit_bytes=8 * 2**20),
        cost_estimate=pl.CostEstimate(
            flops=len(arrays) * rows * width,
            bytes_accessed=4 * len(arrays) * rows * width,
            transcendentals=0,
        ),
    )(*arrays)


def with_partner(slots):
    weights = []
    for low, high in ((0, 2), (3, 3), (4, 4)):
        keys = tuple(k for k in sorted(slots, key=abs) if low <= abs(k) <= high)
        own = stacked([slots[k] for k in keys])
        weights += [(keys, 0, own), (keys, 1, partner(own))]
    return weights


def weight_rows(weights):
    return sum(w.shape[0] * w.shape[1] for _, _, w in weights)


def weight_places(weights):
    return [(keys, other) for keys, other, _ in weights]


def place_weights(places, refs, w_all, first=0):
    me = lax.axis_index("sp")
    pairs = lax.axis_size("sp") // 2
    place, parity = me // 2, lax.rem(me, 2)
    width = w_all.shape[1]
    block_rows = w_all.shape[0] // (2 * pairs)
    for (keys, other), ref in zip(places, refs):
        rows = ref.shape[1]
        for n, k in enumerate(keys):
            block = lax.rem(place + k + pairs, pairs) * 2
            block += 1 - parity if other else parity
            offset = block_rows - rows if k > 0 else 0
            start = pl.multiple_of(block * block_rows + offset, rows)
            w_all[pl.ds(start, rows), :] = ref[n, :, first : first + width]


def prepare_kernel(total_rows, doc_ref, near_ref, far_ref, table_ref, *out_refs):
    tokens = doc_ref.shape[1]
    rows_dev = tokens // GRID_W
    me = lax.axis_index("sp")
    first_row = me * rows_dev
    odd = jnp.full((1, tokens), lax.rem(me, 2), jnp.int32) == 1
    near, own, far = near_ref[...], doc_ref[...], far_ref[...]
    sides = (jnp.where(odd, near, far), own, jnp.where(odd, far, near))
    sides = [side.astype(jnp.float32) for side in sides]
    shape = (GRID_W, LANES)
    col = lax.broadcasted_iota(jnp.int32, shape, 0)
    lane = lax.broadcasted_iota(jnp.int32, shape, 1)
    upper = lane // GRID_W
    key_col = lane - upper * GRID_W
    col_first = jnp.clip(col - NA_COLS // 2, 0, GRID_W - NA_COLS)
    col_fits = (key_col >= col_first) & (key_col < col_first + NA_COLS)
    tiles_side = tokens // LANES
    columns = [
        jnp.broadcast_to(sides[1][:, t * LANES : (t + 1) * LANES], (LANES, LANES)).T
        for t in range(tiles_side)
    ]
    masks = {}
    for i in range(rows_dev):
        row_first = jnp.clip(first_row + i - HALF_ROWS, 0, total_rows - NA_ROWS)
        part = i * GRID_W % LANES
        doc_col = columns[i * GRID_W // LANES][part : part + GRID_W, :]
        for k in range(3 * tiles_side):
            key_row = first_row - HALF_ROWS + 2 * k + upper
            t = k % tiles_side
            doc_row = sides[k // tiles_side][:, t * LANES : (t + 1) * LANES]
            masks[i, k] = (
                col_fits
                & (key_row >= row_first)
                & (key_row < row_first + NA_ROWS)
                & (doc_row == doc_col)
            )
    for layer, out_ref in enumerate(out_refs):

        def per_head(h, carry, layer=layer, out_ref=out_ref):
            lines = [table_ref[layer, h, r : r + 1, :] for r in range(table_ref.shape[2])]
            tiles = []
            for r in range(len(lines) - 1):
                line = lines[r] + pltpu.roll(lines[r + 1], GRID_W, 1)
                line = jnp.broadcast_to(line, shape)
                tiles.append(
                    pltpu.roll(line, LANES - (NA_COLS - 1), 1, stride=1, stride_axis=0)
                )
            for i in range(rows_dev):
                rows = slice(i * GRID_W, (i + 1) * GRID_W)
                for k in range(3 * tiles_side):
                    tile = tiles[2 * k - i + NA_ROWS - 1 - HALF_ROWS]
                    out_ref[h, rows, k * LANES : (k + 1) * LANES] = jnp.where(
                        masks[i, k], tile, MASKED
                    )
            return carry

        lax.fori_loop(0, out_ref.shape[0], per_head, 0)


def prepare(documents, near, far, offset_bias):
    tokens = documents.shape[0]
    total_rows = tokens // GRID_W * lax.axis_size("sp")
    layers, heads, _, cols = offset_bias.shape
    table = jnp.pad(offset_bias, ((0, 0), (0, 0), (0, 0), (0, LANES - cols)))
    size = heads * tokens * 3 * tokens
    return pl.pallas_call(
        functools.partial(prepare_kernel, total_rows),
        out_shape=[jax.ShapeDtypeStruct((heads, tokens, 3 * tokens), jnp.float32)] * layers,
        in_specs=[VMEM] * 4,
        out_specs=[VMEM] * layers,
        name="prepare",
        compiler_params=pltpu.CompilerParams(vmem_limit_bytes=16 * 2**20),
        cost_estimate=pl.CostEstimate(
            flops=4 * layers * size, bytes_accessed=layers * size * 4, transcendentals=0
        ),
    )(documents.reshape(1, tokens), near.reshape(1, tokens), far.reshape(1, tokens), table)


def scale_kernel(first_layer, tokens, *refs):
    if first_layer:
        x_ref, gain_ref, scaled_ref, inverse_ref = refs
    else:
        x_ref, total_ref, gain_ref, scaled_ref, inverse_ref, own_ref, new = refs
    parts, _, width = x_ref.shape
    if not first_layer:
        squares = jnp.zeros((tokens, 1), jnp.float32)
        for j in range(parts):
            total = total_ref[j].astype(jnp.float32)
            squares += jnp.sum(total * total, axis=1, keepdims=True)
        out_inverse = lax.rsqrt(squares / D + EPS)
    squares = jnp.zeros((tokens, 1), jnp.float32)
    for j in range(parts):
        x = x_ref[j, :tokens, :].astype(jnp.float32)
        if not first_layer:
            post = x_ref[j, tokens : tokens + PAD_ROWS, :].astype(jnp.float32)
            post = post[0:1] + post[1:2] + post[2:3]
            x = x + total_ref[j].astype(jnp.float32) * out_inverse * post
            rounded = x.astype(jnp.bfloat16)
            new[j] = rounded
            x = rounded.astype(jnp.float32)
        squares += jnp.sum(x * x, axis=1, keepdims=True)
        scaled_ref[:, j * width : (j + 1) * width] = (x * gain_ref[j]).astype(jnp.bfloat16)
    inverse_ref[...] = lax.rsqrt(squares / D + EPS)
    if not first_layer:
        own_ref[...] = new[lax.axis_index("tp")]


def scale(x_all, total_all, gain, tokens):
    first_layer = total_all is None
    parts, _, width = x_all.shape
    outs = [
        jax.ShapeDtypeStruct((tokens, parts * width), jnp.bfloat16),
        jax.ShapeDtypeStruct((tokens, 1), jnp.float32),
    ]
    args, scratch = [x_all], []
    if not first_layer:
        outs.append(jax.ShapeDtypeStruct((tokens, width), jnp.bfloat16))
        scratch.append(pltpu.VMEM((parts, tokens, width), jnp.bfloat16))
        args.append(total_all)
    args.append(gain.reshape(parts, 1, width))
    return pl.pallas_call(
        functools.partial(scale_kernel, first_layer, tokens),
        out_shape=outs,
        in_specs=[VMEM] * len(args),
        out_specs=[VMEM] * len(outs),
        scratch_shapes=scratch,
        name="scale",
        compiler_params=pltpu.CompilerParams(vmem_limit_bytes=8 * 2**20),
        cost_estimate=pl.CostEstimate(
            flops=8 * tokens * parts * width,
            bytes_accessed=4 * tokens * parts * width * 2,
            transcendentals=tokens,
        ),
    )(*args)


def project_kernel(places, firsts, factor, scaled_ref, inverse_ref, *refs):
    if len(firsts) > 1:
        w_refs, (out_ref, w_other, w_all) = refs[:-3], refs[-3:]
        place_weights(places, w_refs, w_other, firsts[1])
    else:
        w_refs, (out_ref, w_all) = refs[:-2], refs[-2:]
    place_weights(places, w_refs, w_all, firsts[0])
    product = jnp.dot(scaled_ref[...], w_all[...], preferred_element_type=jnp.float32)
    product = (product * inverse_ref[...]).astype(jnp.bfloat16)
    if factor is not None:
        product = product * jnp.asarray(factor, jnp.bfloat16)
    out_ref[...] = product


def project(scaled, inverse, weights, part, columns, firsts, width, factor=None):
    tokens = scaled.shape[0]
    blocks = [w for _, _, w in weights]
    rows = weight_rows(weights)
    outs = [jax.ShapeDtypeStruct((tokens, width), jnp.bfloat16)]
    outs += [jax.ShapeDtypeStruct((rows, width), jnp.bfloat16)] * (len(firsts) - 1)
    return pl.pallas_call(
        functools.partial(project_kernel, weight_places(weights), firsts, factor),
        grid=(1,),
        out_shape=outs,
        in_specs=[VMEM] * 2
        + [
            pl.BlockSpec((*w.shape[:2], columns), lambda i: (0, 0, part)) for w in blocks
        ],
        out_specs=[VMEM] * len(outs),
        scratch_shapes=[pltpu.VMEM((rows, width), jnp.bfloat16)],
        name="project",
        compiler_params=pltpu.CompilerParams(vmem_limit_bytes=16 * 2**20),
        cost_estimate=pl.CostEstimate(
            flops=2 * tokens * rows * width,
            bytes_accessed=2 * rows * width * 2,
            transcendentals=0,
        ),
    )(scaled, inverse, *blocks)


def attend_kernel(q_ref, own_ref, near_ref, far_ref, bias_ref, w_ref, out_ref):
    tokens, width = q_ref.shape
    odd = lax.rem(lax.axis_index("sp"), 2)
    sides = ((own_ref, 1), (near_ref, 2 - 2 * odd), (far_ref, 2 * odd))
    lane = lax.broadcasted_iota(jnp.int32, (tokens, LANES), 1)
    lower = lane < HEAD_DIM
    attended = []
    for pair in range(width // LANES):
        lanes = slice(pair * LANES, (pair + 1) * LANES)
        value_lanes = slice(width + pair * LANES, width + (pair + 1) * LANES)
        queries = q_ref[:, lanes]
        results = []
        for half in range(2):
            chosen = jnp.where(lower if half == 0 else ~lower, queries, 0)
            head = 2 * pair + half
            scores = []
            for side, block in sides:
                start = pl.multiple_of(block * tokens, LANES)
                scores.append(
                    lax.dot_general(
                        chosen,
                        side[:, lanes],
                        (((1,), (1,)), ((), ())),
                        preferred_element_type=jnp.float32,
                    )
                    + bias_ref[head, :, pl.ds(start, tokens)]
                )
            top = jnp.max(
                jnp.maximum(jnp.maximum(scores[0], scores[1]), scores[2]),
                axis=1,
                keepdims=True,
            )
            exps = [jnp.exp(score - top) for score in scores]
            total = jnp.sum(exps[0] + exps[1] + exps[2], axis=1, keepdims=True)
            mixed = sum(
                jnp.dot(
                    e.astype(jnp.bfloat16),
                    side[:, value_lanes],
                    preferred_element_type=jnp.float32,
                )
                for e, (side, _) in zip(exps, sides)
            )
            results.append(mixed / total)
        attended.append(jnp.where(lower, results[0], results[1]).astype(jnp.bfloat16))
    attended = jnp.concatenate(attended, axis=1)
    for n in range(out_ref.shape[0]):
        out_ref[n] = lax.dot_general(
            attended,
            w_ref[n * width : (n + 1) * width, :],
            (((1,), (1,)), ((), ())),
            preferred_element_type=jnp.float32,
        ).astype(jnp.bfloat16)


def attend(queries, own, near, far, bias, w_out):
    tokens, width = queries.shape
    rows = w_out.shape[0]
    heads = width // HEAD_DIM
    return pl.pallas_call(
        attend_kernel,
        out_shape=jax.ShapeDtypeStruct((rows // width, tokens, width), jnp.bfloat16),
        in_specs=[VMEM] * 6,
        out_specs=VMEM,
        name="attend",
        compiler_params=pltpu.CompilerParams(vmem_limit_bytes=20 * 2**20),
        cost_estimate=pl.CostEstimate(
            flops=4 * heads * tokens * 3 * tokens * LANES + 2 * tokens * rows * width,
            bytes_accessed=heads * tokens * 3 * tokens * 4 + rows * width * 2,
            transcendentals=heads * tokens * 3 * tokens,
        ),
    )(queries, own, near, far, bias, w_out)


def summed_kernel(arrived_ref, out_ref):
    total = jnp.sum(arrived_ref[...].astype(jnp.float32), axis=0).astype(jnp.bfloat16)
    for n in range(out_ref.shape[0]):
        out_ref[n] = total


def summed_copies(arrived):
    parts, tokens, width = arrived.shape
    spec = pl.BlockSpec((parts, GRID_W, width), lambda i: (0, i, 0))
    return pl.pallas_call(
        summed_kernel,
        grid=(tokens // GRID_W,),
        out_shape=jax.ShapeDtypeStruct(arrived.shape, arrived.dtype),
        in_specs=[spec],
        out_specs=spec,
        name="summed",
        compiler_params=pltpu.CompilerParams(vmem_limit_bytes=8 * 2**20),
        cost_estimate=pl.CostEstimate(
            flops=2 * parts * tokens * width,
            bytes_accessed=4 * parts * tokens * width,
            transcendentals=0,
        ),
    )(arrived)


def spread_kernel(x_ref, gain_ref, out_ref):
    tokens = x_ref.shape[0]
    rest = gain_ref[...]
    rows = []
    for _ in range(3):
        part = rest.astype(jnp.bfloat16)
        rows.append(part.astype(jnp.float32))
        rest = rest - rows[-1]
    index = lax.broadcasted_iota(jnp.int32, (PAD_ROWS, x_ref.shape[1]), 0)
    tail = jnp.where(index == 0, rows[0], jnp.where(index == 1, rows[1], rows[2]))
    tail = jnp.where(index < 3, tail, 0.0).astype(jnp.bfloat16)
    for n in range(out_ref.shape[0]):
        out_ref[n, :tokens, :] = x_ref[...]
        out_ref[n, tokens:, :] = tail


def spread(x, gain, copies):
    tokens, width = x.shape
    return pl.pallas_call(
        spread_kernel,
        out_shape=jax.ShapeDtypeStruct((copies, tokens + PAD_ROWS, width), x.dtype),
        in_specs=[VMEM] * 2,
        out_specs=VMEM,
        name="spread",
        compiler_params=pltpu.CompilerParams(vmem_limit_bytes=8 * 2**20),
        cost_estimate=pl.CostEstimate(
            flops=0, bytes_accessed=2 * copies * tokens * width, transcendentals=0
        ),
    )(x, gain.reshape(1, width))


def layers(
    stream, documents, q_weight, k_weight, v_weight, out_weight, pre_gain, post_gain, offset_bias
):
    tokens, width = stream.shape

    mats = (k_weight, v_weight, q_weight, out_weight)

    def side_by_side(layer, mats):
        return jnp.concatenate([m[layer] for m in mats], axis=1)

    doc_near, doc_far = partner(documents), across(documents)
    x_copies = spread(stream, post_gain[0], lax.axis_size("tp"))
    x_all = exchange(x_copies, "tp")
    chunk, doc_near, doc_far = lax.optimization_barrier((side_by_side(0, mats), doc_near, doc_far))
    biases = prepare(documents, doc_near, doc_far, offset_bias)
    slots = ring(chunk)
    weights = with_partner(slots)

    def block(layer, scaled, inverse, weights):
        (kv,) = project(scaled, inverse, weights, 0, 2 * width, (0,), 2 * width)
        near = partner(kv)
        far = across(kv)
        queries, w_out = project(
            scaled, inverse, weights, 1, 2 * width, (0, width), width, HEAD_DIM**-0.5
        )
        return attend(queries, kv, near, far, biases[layer], w_out)

    scaled, inverse = scale(x_all, None, pre_gain[0], tokens)
    inverse, mats = lax.optimization_barrier((inverse, mats))
    partial_sums = block(0, scaled, inverse, weights)
    chunk, partial_sums = lax.optimization_barrier(
        (side_by_side(1, mats), partial_sums)
    )
    slots = ring(chunk)
    arrived = exchange(partial_sums, "tp")
    arrived, slots[-2], slots[2] = lax.optimization_barrier((arrived, slots[-2], slots[2]))
    weights = with_partner(slots)
    total_all = exchange(summed_copies(arrived), "tp")
    scaled, inverse, own = scale(x_all, total_all, pre_gain[1], tokens)
    partial_sums = block(1, scaled, inverse, weights)
    own_total = exchange(partial_sums, "tp").astype(jnp.float32).sum(axis=0)
    squares = jnp.sum(own_total * own_total, axis=-1, keepdims=True)
    squares = exchange(copies_for(squares, "tp"), "tp").sum(axis=0)
    out_inverse = lax.rsqrt(squares / D + EPS)
    return (own.astype(jnp.float32) + own_total * out_inverse * post_gain[1]).astype(
        jnp.bfloat16
    )


def solution(mesh):
    in_specs = (
        P(("grp", "sp"), "tp"),
        P(("grp", "sp")),
        P(None, "sp", "tp"),
        P(None, "sp", "tp"),
        P(None, "sp", "tp"),
        P(None, "sp", "tp"),
        P(),
        P(None, "tp"),
        P(None, "tp", None, None),
    )
    out_specs = P(("grp", "sp"), "tp")
    return jax.shard_map(layers, mesh=mesh, in_specs=in_specs, out_specs=out_specs, check_vma=False)
```
